32 devices in a mesh: fs: 16 (over z, y, x), tp: 2 (over core).
Axes of the slice: x: 2, y: 2, z: 4, core: 2. Of those that a mesh axis runs over, the one named last changes fastest.
Arguments:
- tokens: bfloat16 [8192, 2048], P('fs'), may hold values from -6 to 6
- norm_gain: float32 [2048], P('fs'), may hold values from 0.1 to 1.9
- w_gate: float32 [16, 2048, 512], P(None, 'fs', 'tp'), may hold values from -0.125 to 0.125
- w_up: float32 [16, 2048, 512], P(None, 'fs', 'tp'), may hold values from -0.125 to 0.125
- w_down: float32 [16, 2048, 512], P(None, 'fs', 'tp'), may hold values from -0.25 to 0.25
- route_expert: int32 [8192, 2], P('fs'), may hold values from 0 to 15, as said below
- group_prob: float32 [8192], P('fs'), may hold values from 0.25 to 1
- pair_logit: float32 [8192, 2], P('fs'), may hold values from -6 to 6
Outputs:
- new_gate: bfloat16 [16, 2048, 512], P('fs', None, 'tp')
- new_up: bfloat16 [16, 2048, 512], P('fs', None, 'tp')
- new_down: bfloat16 [16, 2048, 512], P('fs', None, 'tp')
- mixed: bfloat16 [8192, 2048], P('fs', 'tp')
The draws below stay inside these ranges and needn't reach their ends.
Inputs may be any that keep to these rules, and one draw needn't show every extreme that they name: `route_expert`: each row names two different experts of one group: for its group g both lie in g * 8 to g * 8 + 7, one of 2 groups. In each aligned block of 512 rows every expert is named by exactly 64 rows, half of them in each column.
All inputs are finite; a program needn't handle non-finite values.
Results may differ from the reference program's by a relative error of at most 0.014.
Values may be sent and summed in bfloat16 or wider, within the bound.
A program may use at most 64 MiB of HBM per device.

```python
import jax
import jax.numpy as jnp
from jax import lax

D = 2048
FF = 512
EPG = 8
TOP = 2
ROWS = 512
EXPERTS = 16
GROUPS = 2
CAP = 64
TOKENS = 8192
N_TP = 2


def draw_route_expert(key, part):
    block_count = TOKENS // ROWS
    half_cap = CAP // 2
    per_group = EPG * half_cap

    def one_block(block_key):
        key_order, key_shift, key_label, key_group = jax.random.split(block_key, 4)
        order = jax.random.permutation(key_order, ROWS)
        position = jnp.arange(ROWS, dtype=jnp.int32)
        group_slot = position // per_group
        within = position % per_group
        first_local = within % EPG
        shifts = jax.random.randint(key_shift, (GROUPS,), 1, EPG)
        second_local = (first_local + shifts[group_slot]) % EPG
        relabel = jax.vmap(lambda label_key: jax.random.permutation(label_key, EPG))(jax.random.split(key_label, GROUPS))
        group_perm = jax.random.permutation(key_group, GROUPS)
        chosen_group = group_perm[group_slot]
        first_expert = chosen_group * EPG + relabel[group_slot, first_local]
        second_expert = chosen_group * EPG + relabel[group_slot, second_local]
        paired = jnp.stack([first_expert, second_expert], axis=1).astype(jnp.int32)
        return jnp.zeros((ROWS, TOP), jnp.int32).at[order].set(paired)
    block_keys = jax.random.split(jax.random.fold_in(key, 7), block_count)
    return jax.vmap(one_block)(block_keys).reshape(TOKENS, TOP)


def levels(own_key, extent, shards, least, top_value):
    def one(axis_at, shards_of):
        draws = jax.random.uniform(jax.random.fold_in(jax.random.fold_in(own_key, 6), axis_at), (shards_of,), jnp.float32, least / len(shards), top_value / len(shards))
        return jnp.repeat(jnp.exp(draws), extent[axis_at] // shards_of).reshape((-1,) + (1,) * (len(extent) - axis_at - 1))

    loudness = one(*shards[0])
    for cut in shards[1:]:
        loudness = loudness * one(*cut)
    return loudness


def gaussian(key, extent, deviation, reach, shards=(), kind=jnp.bfloat16):
    array = jax.random.normal(key, extent, jnp.float32) * deviation
    if len(shards) > 0:
        array = levels(key, extent, shards, -0.22, 0.18) * array
    return jnp.clip(array, min=-reach, max=reach).astype(kind)


def setup_inputs(seed: int = 0) -> dict:
    streams_of = jax.random.split(jax.random.key(seed), 9)
    tokens = gaussian(streams_of[0], (TOKENS, D), 1.0, 6.0, ((0, 16),))
    norm_gain = jnp.clip(1.0 + 0.18 * jax.random.normal(streams_of[1], (D,), jnp.float32), 0.1, 1.9)
    w_gate = gaussian(streams_of[2], (EXPERTS, D, FF), D ** -0.5, 0.125, ((1, 16), (2, 2)), jnp.float32)
    w_up = gaussian(streams_of[3], (EXPERTS, D, FF), D ** -0.5, 0.125, ((1, 16), (2, 2)), jnp.float32)
    w_down = gaussian(streams_of[4], (EXPERTS, D, FF), FF ** -0.5, 0.25, ((1, 16), (2, 2)), jnp.float32)
    route_expert = draw_route_expert(jax.random.fold_in(streams_of[8], 71), 0)
    group_prob = jnp.clip(0.25 + 0.75 * jax.random.uniform(streams_of[6], (TOKENS,), jnp.float32) ** levels(streams_of[6], (TOKENS,), ((0, 16),), -0.2, 0.2), 0.25, 1.0)
    pair_logit = gaussian(streams_of[7], (TOKENS, TOP), 1.5, 6.0, ((0, 16),), jnp.float32)
    return {"tokens": tokens, "norm_gain": norm_gain, "w_gate": w_gate, "w_up": w_up, "w_down": w_down, "route_expert": route_expert, "group_prob": group_prob, "pair_logit": pair_logit}


EPSILON = 1e-06

def reference(tokens, norm_gain, w_gate, w_up, w_down, route_expert, group_prob, pair_logit):
    row_scale = norm_gain[None, :, None]
    new_gate = (w_gate * row_scale).astype(jnp.bfloat16)
    new_up = (w_up * row_scale).astype(jnp.bfloat16)
    new_down = w_down.astype(jnp.bfloat16)
    widened = tokens.astype(jnp.float32)
    normed = (widened * lax.rsqrt(lax.optimization_barrier(jnp.mean(widened * widened, axis=1, keepdims=True)) + EPSILON)).astype(jnp.bfloat16)
    flat_ids = route_expert.reshape(-1).astype(jnp.int32)
    order = jnp.argsort(flat_ids, stable=True).astype(jnp.int32)
    per_expert = flat_ids.shape[0] // EXPERTS
    rows_of = (order // TOP).astype(jnp.int32).reshape(EXPERTS, per_expert)
    block_width = FF // N_TP

    def one_expert(operands):
        row_ids, gate_matrix, up_matrix, down_matrix = operands
        chosen = normed[row_ids]
        gate_pre = jnp.dot(chosen, gate_matrix, preferred_element_type=jnp.float32)
        up_pre = jnp.dot(chosen, up_matrix, preferred_element_type=jnp.float32)
        hidden = lax.optimization_barrier((jax.nn.silu(gate_pre) * up_pre).astype(jnp.bfloat16))
        split_hidden = hidden.astype(jnp.float32).reshape(per_expert, N_TP, block_width)
        split_down = down_matrix.astype(jnp.float32).reshape(D, N_TP, block_width)
        parts = jnp.einsum('rnk,dnk->nrd', split_hidden, split_down).astype(jnp.bfloat16)
        parts = lax.optimization_barrier(parts)
        return lax.optimization_barrier(jnp.sum(parts.astype(jnp.float32), axis=0)).astype(jnp.bfloat16)
    results = lax.map(one_expert, (rows_of, new_gate, new_up, new_down))
    per_slot = jnp.zeros((flat_ids.shape[0], D), jnp.bfloat16).at[order].set(results.reshape(-1, D))
    per_slot = lax.optimization_barrier(per_slot)
    per_slot = per_slot.reshape(TOKENS, TOP, D).astype(jnp.float32)
    logit_gap = pair_logit[:, 0] - pair_logit[:, 1]
    weight_first = group_prob * jax.nn.sigmoid(logit_gap)
    weight_second = group_prob * jax.nn.sigmoid(-logit_gap)
    mixed = (weight_first[:, None] * per_slot[:, 0] + weight_second[:, None] * per_slot[:, 1]).astype(jnp.bfloat16)
    return (new_gate, new_up, new_down, mixed)
```

```python
import functools

import jax
import jax.numpy as jnp
from jax import lax
from jax.experimental import pallas as pl
from jax.experimental.pallas import tpu as pltpu
from jax.sharding import PartitionSpec as P

EPG = 8
TOP = 2
EPSILON = 1e-06
MESH = pl.DeviceIdType.MESH
F32, BF16 = jnp.float32, jnp.bfloat16
CHUNKS = 4
VMEM_LIMIT = 62 * 1024 * 1024


def index_grid(shape, dim):
    return lax.broadcasted_iota(jnp.int32, shape, dim).astype(F32)


def dot(a, b, contract=((1,), (0,)), **kw):
    return lax.dot_general(a, b, (contract, ((), ())), preferred_element_type=F32, **kw)


def send(src, dst, send_sem, recv_sem, **where):
    return pltpu.make_async_remote_copy(
        src_ref=src, dst_ref=dst, send_sem=send_sem, recv_sem=recv_sem, device_id=where, device_id_type=MESH
    )


def partner(me, j, n):
    if n & (n - 1):
        return (me + j) % n
    p, bit = 0, 1
    while bit < n:
        here = (me // bit) % 2
        p = p + bit * (1 - here if j & bit else here)
        bit *= 2
    return p


def kernel(
    n, T, ids, gain, prob, logit, tokens_in, gate_in, up_in, down_in, gate_out, up_out, down_out, mixed_out,
    tokens, w_gate, w_up, w_down, new_gate, new_up, new_down, mixed,
    wb, normed, info_t, s1s, i1s, s1r, i1r, s2s, x, sel, place, hid, ps, pr, eo, ret, ms, fin,
    in_sem, out_sem, w_snd, w_rcv, s1_snd, s1_rcv, i1_snd, i1_rcv, s2_snd, s2_rcv, tp_snd, tp_rcv,
    p_snd, p_rcv, r_snd, r_rcv, f_snd, f_rcv,
):
    me, tpi = lax.axis_index("fs"), lax.axis_index("tp")
    R, D = tokens.shape
    G = n // EPG
    g, i = me // EPG, me % EPG
    Rg, cap, Dt, K = R // G, TOP * R // n, D // T, D // n
    S = EPG * cap
    W = i1s.shape[2]
    C, Dc = ps.shape[1], ps.shape[4]

    barrier = pltpu.get_barrier_semaphore()

    def greet(k, c):
        pl.semaphore_signal(barrier, inc=1, device_id={"fs": (me + k) % n}, device_id_type=MESH)
        return c

    lax.fori_loop(1, n, greet, 0)
    for o in range(1, T):
        pl.semaphore_signal(barrier, inc=1, device_id={"tp": (tpi + o) % T}, device_id_type=MESH)

    loads = [
        pltpu.make_async_copy(src, dst, in_sem.at[k])
        for k, (src, dst) in enumerate(
            ((tokens_in, tokens), (gate_in, w_gate), (up_in, w_up), (down_in, w_down))
        )
    ]
    for load in loads:
        load.start()

    def block(p):
        return pl.ds(pl.multiple_of(p * K, K), K)

    def slots(p):
        return pl.ds(pl.multiple_of(p * cap, cap), cap)

    diagonal = index_grid((K, K), 0) == index_grid((K, K), 1)
    gains = jnp.sum(jnp.where(diagonal, gain[...], 0.0), axis=1, keepdims=True)

    def cast_weights(m, src, scaled):
        def cast(p, c):
            v = src[p]
            wb[m, p] = (v * gains if scaled else v).astype(BF16)
            return c

        loads[1 + m].wait()
        lax.fori_loop(0, n, cast, 0)

    order = [*range(n // 2, n), *range(1, n // 2)]

    def send_weights(m, dst):
        for j in order:
            p = partner(me, j, n)
            send(wb.at[m, p], dst.at[block(me)], w_snd.at[m, p], w_rcv.at[m, me], fs=p).start()
        dst[block(me), :] = wb[m, me]

    def wait_weights(m, dst):
        def body(k, c):
            p = (me + k) % n
            send(wb.at[m, p], dst.at[block(p)], w_snd.at[m, p], w_rcv.at[m, p], fs=p).wait()
            return c

        lax.fori_loop(1, n, body, 0)

    id0, id1 = ids[0:1, :].astype(F32), ids[1:2, :].astype(F32)
    gap = logit[0:1, :] - logit[1:2, :]
    gid = jnp.floor(id0 * (1.0 / EPG))
    experts = index_grid((n, R), 0)
    m0, m1 = experts == id0, experts == id1
    before = jnp.where(index_grid((R, R), 0) < index_grid((R, R), 1), 1.0, 0.0).astype(BF16)
    rank = dot(jnp.where(m0 | m1, 1.0, 0.0).astype(BF16), before)
    in_group = index_grid((max(G, 16), R), 0) == gid
    group_rank = dot(jnp.where(in_group, 1.0, 0.0).astype(BF16), before)
    slot0 = jnp.sum(jnp.where(m0, rank, 0.0), axis=0, keepdims=True) + (id0 - EPG * gid) * cap
    slot1 = jnp.sum(jnp.where(m1, rank, 0.0), axis=0, keepdims=True) + (id1 - EPG * gid) * cap
    pos = jnp.sum(jnp.where(in_group, group_rank, 0.0), axis=0, keepdims=True)
    line = index_grid((8, R), 0)
    table = jnp.zeros((8, R), F32)
    rows = (slot0, slot1, prob[...] * jax.nn.sigmoid(gap), prob[...] * jax.nn.sigmoid(-gap), gid, pos)
    for at, value in enumerate(rows):
        table = jnp.where(line == at, value, table)
    info_t[...] = table.T

    step = 64

    def norm(b, c):
        rows = pl.ds(pl.multiple_of(b * step, step), step)
        v = tokens[rows, :].astype(F32)
        scale = lax.rsqrt(jnp.mean(v * v, axis=1, keepdims=True) + EPSILON)
        part = tokens[rows, pl.ds(pl.multiple_of(tpi * Dt, Dt), Dt)].astype(F32)
        normed[rows, :] = (part * scale).astype(BF16)
        return c

    loads[0].wait()
    lax.fori_loop(0, R // step, norm, 0)

    for k in range(G):
        q = (g + 1 + k) % G
        pick = jnp.where((index_grid((W, R), 0) == pos) & (gid == q.astype(F32)), 1.0, 0.0)
        info_q = dot(table, pick, ((1,), (1,)), precision=lax.Precision.HIGHEST)
        rows_q = dot(pick[:Rg].astype(BF16), normed[...]).astype(BF16)
        if k == G - 1:
            s1r[g] = rows_q
            i1r[g] = info_q
        else:
            s1s[q] = rows_q
            i1s[q] = info_q

    cast_weights(0, w_gate, True)
    pl.semaphore_wait(barrier, n - 1 + T - 1)

    for k in range(G - 1):
        q = (g + 1 + k) % G
        send(i1s.at[q], i1r.at[g], i1_snd.at[q], i1_rcv.at[g], fs=q * EPG + i).start()
        send(s1s.at[q], s1r.at[g], s1_snd.at[q], s1_rcv.at[g], fs=q * EPG + i).start()
    send_weights(0, new_gate)

    def dispatch(h):
        slot_q = i1r[h]
        grid = index_grid((S, Rg), 0)
        spread = (grid == slot_q[0:1, :Rg]) | (grid == slot_q[1:2, :Rg])
        s2s[h] = dot(jnp.where(spread, 1.0, 0.0).astype(BF16), s1r[h]).astype(BF16)
        for j in range(1, EPG):
            p = partner(i, j, EPG)
            send(
                s2s.at[h, slots(p)], x.at[tpi, h, slots(i)], s2_snd.at[h, p], s2_rcv.at[h, i], fs=g * EPG + p
            ).start()
        x[tpi, h, slots(i), :] = s2s[h, slots(i), :]

    dispatch(g)
    cast_weights(1, w_up, True)
    send_weights(1, new_up)
    cast_weights(2, w_down, False)

    for k in range(G - 1):
        h = (g + 1 + k) % G
        send(i1s.at[h], i1r.at[h], i1_snd.at[h], i1_rcv.at[h], fs=h * EPG + i).wait()
        send(s1s.at[h], s1r.at[h], s1_snd.at[h], s1_rcv.at[h], fs=h * EPG + i).wait()
        dispatch(h)
    send_weights(2, new_down)

    for k in range(G):
        h = (g + 1 + k) % G
        cols = i1r[h].T[:Rg]
        grid = index_grid((Rg, S), 1)
        for c in range(TOP):
            sel[h, c] = jnp.where(grid == cols[:, c : c + 1], 1.0, 0.0).astype(BF16)
        grid = index_grid((R, Rg), 1)
        here = (grid == info_t[:, 5:6]) & (info_t[:, 4:5] == h.astype(F32))
        place[h] = jnp.where(here, 1.0, 0.0).astype(BF16)

    for k in (G - 1, *range(G - 1)):
        h = (g + 1 + k) % G
        for j in range(1, EPG):
            p = (i + j) % EPG
            send(
                s2s.at[h, slots(p)], x.at[tpi, h, slots(p)], s2_snd.at[h, p], s2_rcv.at[h, p], fs=g * EPG + p
            ).wait()
        for o in range(1, T):
            send(x.at[tpi, h], x.at[tpi, h], tp_snd.at[h, o], tp_rcv.at[h, o], tp=(tpi + o) % T).start()
    for k in range(G):
        h = (g + 1 + k) % G
        for o in range(1, T):
            t = (tpi + T - o) % T
            send(x.at[t, h], x.at[t, h], tp_snd.at[h, o], tp_rcv.at[h, o], tp=(tpi + o) % T).wait()

    stores = [
        pltpu.make_async_copy(src, dst, out_sem.at[k])
        for k, (src, dst) in enumerate(((new_gate, gate_out), (new_up, up_out), (new_down, down_out)))
    ]
    wait_weights(0, new_gate)
    stores[0].start()
    wait_weights(1, new_up)
    stores[1].start()

    tile = min(S, 256)
    for k in range(G):
        h = (g + 1 + k) % G

        def expert(b, c):
            rows = pl.ds(pl.multiple_of(b * tile, tile), tile)
            gate_pre = up_pre = 0.0
            for t in range(T):
                part = x[t, h, rows, :]
                gate_pre += dot(part, new_gate[t * Dt : (t + 1) * Dt, :])
                up_pre += dot(part, new_up[t * Dt : (t + 1) * Dt, :])
            hid[h, rows, :] = (gate_pre / (1.0 + jnp.exp(-gate_pre)) * up_pre).astype(BF16)
            return c

        lax.fori_loop(0, S // tile, expert, 0)

    wait_weights(2, new_down)
    stores[2].start()

    def sum_units(c, h):
        for t in range(T):
            at = t * Dt + c * Dc
            ps[t, c, h] = dot(hid[h], new_down[at : at + Dc, :], ((1,), (1,))).astype(BF16)
        for o in range(1, T):
            t = (tpi + o) % T
            send(ps.at[t, c, h], pr.at[o, c, h], p_snd.at[c, h, o], p_rcv.at[c, h, o], tp=t).start()

    def hand_back(c, h):
        total = ps[tpi, c, h].astype(F32)
        for o in range(1, T):
            t = (tpi + o) % T
            send(ps.at[t, c, h], pr.at[o, c, h], p_snd.at[c, h, o], p_rcv.at[c, h, o], tp=t).wait()
            total += pr[o, c, h].astype(F32)
        eo[c, h] = total.astype(BF16)
        for j in range(1, EPG):
            p = partner(i, j, EPG)
            send(
                eo.at[c, h, slots(p)], ret.at[c, h, slots(i)], r_snd.at[c, h, p], r_rcv.at[c, h, i], fs=g * EPG + p
            ).start()
        ret[c, h, slots(i), :] = eo[c, h, slots(i), :]

    def mix(c, h, last):
        for j in range(1, EPG):
            p = (i + j) % EPG
            send(
                eo.at[c, h, slots(p)], ret.at[c, h, slots(p)], r_snd.at[c, h, p], r_rcv.at[c, h, p], fs=g * EPG + p
            ).wait()
        cols = i1r[h].T[:Rg]
        outs = ret[c, h]
        both = (cols[:, 2:3] * dot(sel[h, 0], outs) + cols[:, 3:4] * dot(sel[h, 1], outs)).astype(BF16)
        if last:
            fin[c, g] = both
        else:
            ms[c, h] = both
            send(ms.at[c, h], fin.at[c, g], f_snd.at[c, h], f_rcv.at[c, g], fs=h * EPG + i).start()

    steps = [(c, (g + 1 + k) % G, k == G - 1) for k in range(G) for c in range(C)]
    for s in range(len(steps) + 3):
        if s < len(steps):
            sum_units(*steps[s][:2])
        if 1 <= s <= len(steps):
            hand_back(*steps[s - 1][:2])
        if s >= 3:
            mix(*steps[s - 3])

    for c in range(C):
        total = 0.0
        for k in (G - 1, *range(G - 1)):
            q = (g + 1 + k) % G
            if k < G - 1:
                send(ms.at[c, q], fin.at[c, q], f_snd.at[c, q], f_rcv.at[c, q], fs=q * EPG + i).wait()
            total += dot(place[q], fin[c, q])
        mixed[:, c * Dc : (c + 1) * Dc] = total.astype(BF16)
        stores.append(
            pltpu.make_async_copy(
                mixed.at[:, c * Dc : (c + 1) * Dc], mixed_out.at[:, c * Dc : (c + 1) * Dc], out_sem.at[3 + c]
            )
        )
        stores[-1].start()
    for store in stores:
        store.wait()


def hand_over(count, *refs):
    sources, results, rooms = refs[:4], refs[4:8], refs[8:12]
    arrived, left = refs[12:]
    into, out = [], []
    for a, (source, room, result) in enumerate(zip(sources, rooms, results)):
        height = source.shape[0] // count
        for b in range(count):
            rows = pl.ds(b * height, height)
            into.append(pltpu.make_async_copy(source.at[rows], room.at[rows], arrived.at[a, b]))
            out.append(pltpu.make_async_copy(room.at[rows], result.at[rows], left.at[a, b]))
    for copy in into:
        copy.start()
    for first, second in zip(into, out):
        first.wait()
        second.start()
    for copy in out:
        copy.wait()


def local(tokens, norm_gain, w_gate, w_up, w_down, route_expert, group_prob, pair_logit):
    n, T = lax.axis_size("fs"), lax.axis_size("tp")
    R, D = tokens.shape
    F = w_gate.shape[2]
    G = n // EPG
    Rg, cap, Dt = R // G, TOP * R // n, D // T
    S, W = EPG * cap, max(Rg, 128)
    Dc = min(Dt, max(Dt // CHUNKS, 128))
    C = Dt // Dc
    vmem = pl.BlockSpec(memory_space=pltpu.VMEM)
    hbm = pl.BlockSpec(memory_space=pl.ANY)
    sem = pltpu.SemaphoreType.DMA
    weights = jax.ShapeDtypeStruct((D, F), BF16)
    shapes = [weights, weights, weights, jax.ShapeDtypeStruct((R, Dt), BF16)]
    results = pl.pallas_call(
        functools.partial(kernel, n, T),
        out_shape=shapes,
        in_specs=[vmem] * 4 + [hbm] * 4,
        out_specs=[hbm] * 4,
        scratch_shapes=[
            pltpu.VMEM((R, D), BF16),
            pltpu.VMEM(w_gate.shape, F32),
            pltpu.VMEM(w_up.shape, F32),
            pltpu.VMEM(w_down.shape, F32),
            pltpu.VMEM((D, F), BF16),
            pltpu.VMEM((D, F), BF16),
            pltpu.VMEM((D, F), BF16),
            pltpu.VMEM((R, Dt), BF16),
            pltpu.VMEM((3, n, D // n, F), BF16),
            pltpu.VMEM((R, Dt), BF16),
            pltpu.VMEM((R, 8), F32),
            pltpu.VMEM((G, Rg, Dt), BF16),
            pltpu.VMEM((G, 8, W), F32),
            pltpu.VMEM((G, Rg, Dt), BF16),
            pltpu.VMEM((G, 8, W), F32),
            pltpu.VMEM((G, S, Dt), BF16),
            pltpu.VMEM((T, G, S, Dt), BF16),
            pltpu.VMEM((G, TOP, Rg, S), BF16),
            pltpu.VMEM((G, R, Rg), BF16),
            pltpu.VMEM((G, S, F), BF16),
            pltpu.VMEM((T, C, G, S, Dc), BF16),
            pltpu.VMEM((T, C, G, S, Dc), BF16),
            pltpu.VMEM((C, G, S, Dc), BF16),
            pltpu.VMEM((C, G, S, Dc), BF16),
            pltpu.VMEM((C, G, Rg, Dc), BF16),
            pltpu.VMEM((C, G, Rg, Dc), BF16),
            sem((4,)), sem((3 + C,)),
            sem((3, n)), sem((3, n)),
            sem((G,)), sem((G,)), sem((G,)), sem((G,)),
            sem((G, EPG)), sem((G, EPG)),
            sem((G, T)), sem((G, T)), sem((C, G, T)), sem((C, G, T)),
            sem((C, G, EPG)), sem((C, G, EPG)),
            sem((C, G)), sem((C, G)),
        ],
        compiler_params=pltpu.CompilerParams(
            collective_id=0, has_side_effects=True, vmem_limit_bytes=VMEM_LIMIT
        ),
    )(
        route_expert.T, norm_gain[None, :], group_prob[None, :], pair_logit.T,
        tokens, w_gate, w_up, w_down,
    )
    parts = 2
    gate, up, down, mixed = pl.pallas_call(
        functools.partial(hand_over, parts),
        out_shape=shapes,
        in_specs=[hbm] * 4,
        out_specs=[hbm] * 4,
        scratch_shapes=[pltpu.VMEM(s.shape, s.dtype) for s in shapes] + [sem((4, parts)), sem((4, parts))],
    )(*results)
    return gate[None], up[None], down[None], mixed


def solution(mesh):
    placed = (
        P("fs", None),
        P("fs"),
        P(None, "fs", "tp"),
        P(None, "fs", "tp"),
        P(None, "fs", "tp"),
        P("fs", None),
        P("fs"),
        P("fs", None),
    )
    return jax.shard_map(
        local,
        mesh=mesh,
        in_specs=placed,
        out_specs=(P("fs", None, "tp"), P("fs", None, "tp"), P("fs", None, "tp"), P("fs", "tp")),
        check_vma=False,
    )
```

```python
import functools

import jax
import jax.numpy as jnp
from jax import lax
from jax.experimental import pallas as pl
from jax.experimental.pallas import tpu as pltpu
from jax.sharding import PartitionSpec as P

EPG = 8
TOP = 2
EPSILON = 1e-06
MESH = pl.DeviceIdType.MESH
F32, BF16 = jnp.float32, jnp.bfloat16
CHUNKS = 4
VMEM_LIMIT = 62 * 1024 * 1024


def index_grid(shape, dim):
    return lax.broadcasted_iota(jnp.int32, shape, dim).astype(F32)


def dot(a, b, contract=((1,), (0,)), **kw):
    return lax.dot_general(a, b, (contract, ((), ())), preferred_element_type=F32, **kw)


def send(src, dst, send_sem, recv_sem, **where):
    return pltpu.make_async_remote_copy(
        src_ref=src, dst_ref=dst, send_sem=send_sem, recv_sem=recv_sem, device_id=where, device_id_type=MESH
    )


def partner(me, j, n):
    if n & (n - 1):
        return (me + j) % n
    p, bit = 0, 1
    while bit < n:
        here = (me // bit) % 2
        p = p + bit * (1 - here if j & bit else here)
        bit *= 2
    return p


def kernel(
    n, T, ids, gain, prob, logit, tokens_in, gate_in, up_in, down_in, gate_out, up_out, down_out, mixed_out,
    tokens, w_gate, w_up, w_down, new_gate, new_up, new_down, mixed,
    wb, normed, info_t, s1s, i1s, s1r, i1r, s2s, x, sel, place, hid, ps, pr, eo, ret, ms, fin,
    in_sem, out_sem, w_snd, w_rcv, s1_snd, s1_rcv, i1_snd, i1_rcv, s2_snd, s2_rcv, tp_snd, tp_rcv,
    p_snd, p_rcv, r_snd, r_rcv, f_snd, f_rcv,
):
    me, tpi = lax.axis_index("fs"), lax.axis_index("tp")
    R, D = tokens.shape
    G = n // EPG
    g, i = me // EPG, me % EPG
    Rg, cap, Dt, K = R // G, TOP * R // n, D // T, D // n
    S = EPG * cap
    W = i1s.shape[2]
    C, Dc = ps.shape[1], ps.shape[4]

    barrier = pltpu.get_barrier_semaphore()

    def greet(k, c):
        pl.semaphore_signal(barrier, inc=1, device_id={"fs": (me + k) % n}, device_id_type=MESH)
        return c

    lax.fori_loop(1, n, greet, 0)
    for o in range(1, T):
        pl.semaphore_signal(barrier, inc=1, device_id={"tp": (tpi + o) % T}, device_id_type=MESH)

    loads = [
        pltpu.make_async_copy(src, dst, in_sem.at[k])
        for k, (src, dst) in enumerate(
            ((tokens_in, tokens), (gate_in, w_gate), (up_in, w_up), (down_in, w_down))
        )
    ]
    for load in loads:
        load.start()

    def block(p):
        return pl.ds(pl.multiple_of(p * K, K), K)

    def slots(p):
        return pl.ds(pl.multiple_of(p * cap, cap), cap)

    diagonal = index_grid((K, K), 0) == index_grid((K, K), 1)
    gains = jnp.sum(jnp.where(diagonal, gain[...], 0.0), axis=1, keepdims=True)

    def cast_weights(m, src, scaled):
        def cast(p, c):
            v = src[p]
            wb[m, p] = (v * gains if scaled else v).astype(BF16)
            return c

        loads[1 + m].wait()
        lax.fori_loop(0, n, cast, 0)

    def send_weights(m, dst, order):
        for j in order:
            p = partner(me, j, n)
            send(wb.at[m, p], dst.at[block(me)], w_snd.at[m, p], w_rcv.at[m, me], fs=p).start()

    near, far = range(1, EPG), range(EPG, n)

    def weights_from(m, dst, p):
        return send(wb.at[m, p], dst.at[block(p)], w_snd.at[m, p], w_rcv.at[m, p], fs=p)

    def wait_weights(m, dst, first, count):
        def body(k, c):
            p = first + k

            @pl.when(p != me)
            def _():
                weights_from(m, dst, p).wait_recv()

            return c

        lax.fori_loop(0, count, body, 0)

    id0, id1 = ids[0:1, :].astype(F32), ids[1:2, :].astype(F32)
    gap = logit[0:1, :] - logit[1:2, :]
    gid = jnp.floor(id0 * (1.0 / EPG))
    experts = index_grid((n, R), 0)
    m0, m1 = experts == id0, experts == id1
    before = jnp.where(index_grid((R, R), 0) < index_grid((R, R), 1), 1.0, 0.0).astype(BF16)
    rank = dot(jnp.where(m0 | m1, 1.0, 0.0).astype(BF16), before)
    in_group = index_grid((max(G, 16), R), 0) == gid
    group_rank = dot(jnp.where(in_group, 1.0, 0.0).astype(BF16), before)
    slot0 = jnp.sum(jnp.where(m0, rank, 0.0), axis=0, keepdims=True) + (id0 - EPG * gid) * cap
    slot1 = jnp.sum(jnp.where(m1, rank, 0.0), axis=0, keepdims=True) + (id1 - EPG * gid) * cap
    pos = jnp.sum(jnp.where(in_group, group_rank, 0.0), axis=0, keepdims=True)
    line = index_grid((8, R), 0)
    table = jnp.zeros((8, R), F32)
    rows = (slot0, slot1, prob[...] * jax.nn.sigmoid(gap), prob[...] * jax.nn.sigmoid(-gap), gid, pos)
    for at, value in enumerate(rows):
        table = jnp.where(line == at, value, table)
    info_t[...] = table.T

    step = 64

    def norm(b, c):
        rows = pl.ds(pl.multiple_of(b * step, step), step)
        v = tokens[rows, :].astype(F32)
        scale = lax.rsqrt(jnp.mean(v * v, axis=1, keepdims=True) + EPSILON)
        part = tokens[rows, pl.ds(pl.multiple_of(tpi * Dt, Dt), Dt)].astype(F32)
        normed[rows, :] = (part * scale).astype(BF16)
        return c

    loads[0].wait()
    lax.fori_loop(0, R // step, norm, 0)

    for k in range(G):
        q = (g + 1 + k) % G
        pick = jnp.where((index_grid((W, R), 0) == pos) & (gid == q.astype(F32)), 1.0, 0.0)
        info_q = dot(table, pick, ((1,), (1,)), precision=lax.Precision.HIGHEST)
        rows_q = dot(pick[:Rg].astype(BF16), normed[...]).astype(BF16)
        if k == G - 1:
            s1r[g] = rows_q
            i1r[g] = info_q
        else:
            s1s[q] = rows_q
            i1s[q] = info_q

    cast_weights(0, w_gate, True)
    pl.semaphore_wait(barrier, n - 1 + T - 1)

    for k in range(G - 1):
        q = (g + 1 + k) % G
        send(i1s.at[q], i1r.at[g], i1_snd.at[q], i1_rcv.at[g], fs=q * EPG + i).start()
        send(s1s.at[q], s1r.at[g], s1_snd.at[q], s1_rcv.at[g], fs=q * EPG + i).start()

    def dispatch(h):
        slot_q = i1r[h]
        grid = index_grid((S, Rg), 0)
        spread = (grid == slot_q[0:1, :Rg]) | (grid == slot_q[1:2, :Rg])
        s2s[h] = dot(jnp.where(spread, 1.0, 0.0).astype(BF16), s1r[h]).astype(BF16)
        for j in range(1, EPG):
            p = partner(i, j, EPG)
            send(
                s2s.at[h, slots(p)], x.at[tpi, h, slots(i)], s2_snd.at[h, p], s2_rcv.at[h, i], fs=g * EPG + p
            ).start()
        x[tpi, h, slots(i), :] = s2s[h, slots(i), :]

    dispatch(g)
    send_weights(0, new_gate, far)
    cast_weights(1, w_up, True)
    send_weights(1, new_up, far)
    send_weights(0, new_gate, near)
    send_weights(1, new_up, near)
    cast_weights(2, w_down, False)
    for m, dst in enumerate((new_gate, new_up, new_down)):
        dst[block(me), :] = wb[m, me]

    for k in range(G - 1):
        h = (g + 1 + k) % G
        send(i1s.at[h], i1r.at[h], i1_snd.at[h], i1_rcv.at[h], fs=h * EPG + i).wait()
        send(s1s.at[h], s1r.at[h], s1_snd.at[h], s1_rcv.at[h], fs=h * EPG + i).wait()
        dispatch(h)
    send_weights(2, new_down, near)
    send_weights(2, new_down, far)

    for k in range(G):
        h = (g + 1 + k) % G
        cols = i1r[h].T[:Rg]
        grid = index_grid((Rg, S), 1)
        for c in range(TOP):
            sel[h, c] = jnp.where(grid == cols[:, c : c + 1], 1.0, 0.0).astype(BF16)
        grid = index_grid((R, Rg), 1)
        here = (grid == info_t[:, 5:6]) & (info_t[:, 4:5] == h.astype(F32))
        place[h] = jnp.where(here, 1.0, 0.0).astype(BF16)

    def exchange(h):
        for j in range(1, EPG):
            p = partner(i, j, EPG)
            send(
                s2s.at[h, slots(p)], x.at[tpi, h, slots(p)], s2_snd.at[h, p], s2_rcv.at[h, p], fs=g * EPG + p
            ).wait_recv()
        for o in range(1, T):
            send(x.at[tpi, h], x.at[tpi, h], tp_snd.at[h, o], tp_rcv.at[h, o], tp=(tpi + o) % T).start()

    def exchanged(h):
        for o in range(1, T):
            t = (tpi + T - o) % T
            send(x.at[t, h], x.at[t, h], tp_snd.at[h, o], tp_rcv.at[h, o], tp=(tpi + o) % T).wait_recv()

    tile = min(S, 256)

    def apply_experts(h):
        def expert(b, c):
            rows = pl.ds(pl.multiple_of(b * tile, tile), tile)
            gate_pre = up_pre = 0.0
            for t in range(T):
                part = x[t, h, rows, :]
                gate_pre += dot(part, new_gate[t * Dt : (t + 1) * Dt, :])
                up_pre += dot(part, new_up[t * Dt : (t + 1) * Dt, :])
            hid[h, rows, :] = (gate_pre / (1.0 + jnp.exp(-gate_pre)) * up_pre).astype(BF16)
            return c

        lax.fori_loop(0, S // tile, expert, 0)

    stores = [
        pltpu.make_async_copy(src, dst, out_sem.at[k])
        for k, (src, dst) in enumerate(((new_gate, gate_out), (new_up, up_out), (new_down, down_out)))
    ]
    others = [(g + 1 + k) % G for k in range(G - 1)]
    exchange(g)
    for h in others:
        exchange(h)
    wait_weights(0, new_gate, 0, n)
    stores[0].start()
    wait_weights(1, new_up, 0, n)
    stores[1].start()
    exchanged(g)
    apply_experts(g)
    for h in others:
        exchanged(h)
        apply_experts(h)

    def partial(h, c, o, t):
        return send(ps.at[o, c, h], pr.at[o, c, h], p_snd.at[c, h, o], p_rcv.at[c, h, o], tp=t)

    def sum_units(t, o, c, h):
        rows = pl.ds(pl.multiple_of(t * Dt + c * Dc, Dc), Dc)
        ps[o, c, h] = dot(hid[h], new_down[rows, :], ((1,), (1,))).astype(BF16)

        @pl.when(t != tpi)
        def _():
            partial(h, c, o, t).start()

    def return_to(h, c, p, q):
        return send(
            eo.at[c, h, slots(p)], ret.at[c, h, slots(q)], r_snd.at[c, h, p], r_rcv.at[c, h, q], fs=g * EPG + p
        )

    def hand_back(c, h):
        total = ps[0, c, h].astype(F32)
        for o in range(1, T):
            partial(h, c, o, (tpi + o) % T).wait_recv()
            total += pr[o, c, h].astype(F32)
        eo[c, h] = total.astype(BF16)
        for j in range(1, EPG):
            return_to(h, c, partner(i, j, EPG), i).start()
        ret[c, h, slots(i), :] = eo[c, h, slots(i), :]

    def result_to(h, c, q):
        return send(ms.at[c, h], fin.at[c, q], f_snd.at[c, h], f_rcv.at[c, q], fs=h * EPG + i)

    def mix(c, h, last):
        for j in range(1, EPG):
            p = partner(i, j, EPG)
            return_to(h, c, p, p).wait_recv()
        cols = i1r[h].T[:Rg]
        outs = ret[c, h]
        both = (cols[:, 2:3] * dot(sel[h, 0], outs) + cols[:, 3:4] * dot(sel[h, 1], outs)).astype(BF16)
        if last:
            fin[c, g] = both
        else:
            ms[c, h] = both
            result_to(h, c, g).start()

    first = (me * T) // n
    for k in range(T):
        t = (first + k) % T
        wait_weights(2, new_down, t * (n // T), n // T)
        if k == T - 1:
            stores[2].start()
        for h in (*others, g):
            for c in range(C):
                sum_units(t, (t - tpi + T) % T, c, h)

        @pl.when(t == tpi)
        def _():
            for h in (*others, g):
                for c in range(C):
                    hand_back(c, h)
            for h in others:
                for c in range(C):
                    mix(c, h, False)

    for c in range(C):
        mix(c, g, True)

    for c in range(C):
        total = 0.0
        for k in (G - 1, *range(G - 1)):
            q = (g + 1 + k) % G
            if k < G - 1:
                result_to(q, c, q).wait_recv()
            total += dot(place[q], fin[c, q])
        mixed[:, c * Dc : (c + 1) * Dc] = total.astype(BF16)
        stores.append(
            pltpu.make_async_copy(
                mixed.at[:, c * Dc : (c + 1) * Dc], mixed_out.at[:, c * Dc : (c + 1) * Dc], out_sem.at[3 + c]
            )
        )
        stores[-1].start()
    for store in stores:
        store.wait()

    def drain(k, c):
        p = (me + k) % n
        for m, dst in enumerate((new_gate, new_up, new_down)):
            weights_from(m, dst, p).wait_send()
        return c

    lax.fori_loop(1, n, drain, 0)
    for h in (*others, g):
        for o in range(1, T):
            send(x.at[tpi, h], x.at[tpi, h], tp_snd.at[h, o], tp_rcv.at[h, o], tp=(tpi + o) % T).wait_send()
        for j in range(1, EPG):
            p = partner(i, j, EPG)
            send(
                s2s.at[h, slots(p)], x.at[tpi, h, slots(p)], s2_snd.at[h, p], s2_rcv.at[h, p], fs=g * EPG + p
            ).wait_send()
        for c in range(C):
            for o in range(1, T):
                partial(h, c, o, (tpi + o) % T).wait_send()
            for j in range(1, EPG):
                p = partner(i, j, EPG)
                return_to(h, c, p, p).wait_send()
    for h in others:
        for c in range(C):
            result_to(h, c, h).wait_send()


def hand_over(count, *refs):
    sources, results, rooms = refs[:4], refs[4:8], refs[8:12]
    arrived, left = refs[12:]
    into, out = [], []
    for a, (source, room, result) in enumerate(zip(sources, rooms, results)):
        height = source.shape[0] // count
        for b in range(count):
            rows = pl.ds(b * height, height)
            into.append(pltpu.make_async_copy(source.at[rows], room.at[rows], arrived.at[a, b]))
            out.append(pltpu.make_async_copy(room.at[rows], result.at[rows], left.at[a, b]))
    for copy in into:
        copy.start()
    for first, second in zip(into, out):
        first.wait()
        second.start()
    for copy in out:
        copy.wait()


def local(tokens, norm_gain, w_gate, w_up, w_down, route_expert, group_prob, pair_logit):
    n, T = lax.axis_size("fs"), lax.axis_size("tp")
    R, D = tokens.shape
    F = w_gate.shape[2]
    G = n // EPG
    Rg, cap, Dt = R // G, TOP * R // n, D // T
    S, W = EPG * cap, max(Rg, 128)
    Dc = min(Dt, max(Dt // CHUNKS, 128))
    C = Dt // Dc
    vmem = pl.BlockSpec(memory_space=pltpu.VMEM)
    hbm = pl.BlockSpec(memory_space=pl.ANY)
    sem = pltpu.SemaphoreType.DMA
    weights = jax.ShapeDtypeStruct((D, F), BF16)
    shapes = [weights, weights, weights, jax.ShapeDtypeStruct((R, Dt), BF16)]
    results = pl.pallas_call(
        functools.partial(kernel, n, T),
        out_shape=shapes,
        in_specs=[vmem] * 4 + [hbm] * 4,
        out_specs=[hbm] * 4,
        scratch_shapes=[
            pltpu.VMEM((R, D), BF16),
            pltpu.VMEM(w_gate.shape, F32),
            pltpu.VMEM(w_up.shape, F32),
            pltpu.VMEM(w_down.shape, F32),
            pltpu.VMEM((D, F), BF16),
            pltpu.VMEM((D, F), BF16),
            pltpu.VMEM((D, F), BF16),
            pltpu.VMEM((R, Dt), BF16),
            pltpu.VMEM((3, n, D // n, F), BF16),
            pltpu.VMEM((R, Dt), BF16),
            pltpu.VMEM((R, 8), F32),
            pltpu.VMEM((G, Rg, Dt), BF16),
            pltpu.VMEM((G, 8, W), F32),
            pltpu.VMEM((G, Rg, Dt), BF16),
            pltpu.VMEM((G, 8, W), F32),
            pltpu.VMEM((G, S, Dt), BF16),
            pltpu.VMEM((T, G, S, Dt), BF16),
            pltpu.VMEM((G, TOP, Rg, S), BF16),
            pltpu.VMEM((G, R, Rg), BF16),
            pltpu.VMEM((G, S, F), BF16),
            pltpu.VMEM((T, C, G, S, Dc), BF16),
            pltpu.VMEM((T, C, G, S, Dc), BF16),
            pltpu.VMEM((C, G, S, Dc), BF16),
            pltpu.VMEM((C, G, S, Dc), BF16),
            pltpu.VMEM((C, G, Rg, Dc), BF16),
            pltpu.VMEM((C, G, Rg, Dc), BF16),
            sem((4,)), sem((3 + C,)),
            sem((3, n)), sem((3, n)),
            sem((G,)), sem((G,)), sem((G,)), sem((G,)),
            sem((G, EPG)), sem((G, EPG)),
            sem((G, T)), sem((G, T)), sem((C, G, T)), sem((C, G, T)),
            sem((C, G, EPG)), sem((C, G, EPG)),
            sem((C, G)), sem((C, G)),
        ],
        compiler_params=pltpu.CompilerParams(
            collective_id=0, has_side_effects=True, vmem_limit_bytes=VMEM_LIMIT
        ),
    )(
        route_expert.T, norm_gain[None, :], group_prob[None, :], pair_logit.T,
        tokens, w_gate, w_up, w_down,
    )
    parts = 2
    gate, up, down, mixed = pl.pallas_call(
        functools.partial(hand_over, parts),
        out_shape=shapes,
        in_specs=[hbm] * 4,
        out_specs=[hbm] * 4,
        scratch_shapes=[pltpu.VMEM(s.shape, s.dtype) for s in shapes] + [sem((4, parts)), sem((4, parts))],
    )(*results)
    return gate[None], up[None], down[None], mixed


def solution(mesh):
    placed = (
        P("fs", None),
        P("fs"),
        P(None, "fs", "tp"),
        P(None, "fs", "tp"),
        P(None, "fs", "tp"),
        P("fs", None),
        P("fs"),
        P("fs", None),
    )
    return jax.shard_map(
        local,
        mesh=mesh,
        in_specs=placed,
        out_specs=(P("fs", None, "tp"), P("fs", None, "tp"), P("fs", None, "tp"), P("fs", "tp")),
        check_vma=False,
    )
```

```python
import functools

import jax
import jax.numpy as jnp
from jax import lax
from jax.experimental import pallas as pl
from jax.experimental.pallas import tpu as pltpu
from jax.sharding import PartitionSpec as P

EPG = 8
SIDES = 2
TOP = 2
EPSILON = 1e-06
MESH = pl.DeviceIdType.MESH
F32, BF16 = jnp.float32, jnp.bfloat16
CHUNKS = 4
FAR_AFTER = 1
VMEM_LIMIT = 62 * 1024 * 1024


def index_grid(shape, dim):
    return lax.broadcasted_iota(jnp.int32, shape, dim).astype(F32)


def dot(a, b, contract=((1,), (0,)), **kw):
    return lax.dot_general(a, b, (contract, ((), ())), preferred_element_type=F32, **kw)


def send(src, dst, send_sem, recv_sem, **where):
    return pltpu.make_async_remote_copy(
        src_ref=src, dst_ref=dst, send_sem=send_sem, recv_sem=recv_sem, device_id=where, device_id_type=MESH
    )


def partner(me, j, n):
    if n & (n - 1):
        return (me + j) % n
    p, bit = 0, 1
    while bit < n:
        here = (me // bit) % 2
        p = p + bit * (1 - here if j & bit else here)
        bit *= 2
    return p


def kernel(
    n, T, ids, gain, prob, logit, tokens_in, gate_in, up_in, down_in, gate_out, up_out, down_out, mixed_out,
    tokens, w_gate, w_up, w_down, new_gate, new_up, new_down, mixed,
    wb, normed, info_t, s1s, i1s, s1r, i1r, s2s, x, sel, place, hid, ps, pr, eo, ret, ms, fin,
    in_sem, out_sem, w_snd, w_rcv, s1_snd, s1_rcv, i1_snd, i1_rcv, s2_snd, s2_rcv, tp_snd, tp_rcv,
    p_snd, p_rcv, r_snd, r_rcv, f_snd, f_rcv,
):
    me, tpi = lax.axis_index("fs"), lax.axis_index("tp")
    R, D = tokens.shape
    G = n // EPG
    g, i = me // EPG, me % EPG
    Rg, cap, Dt, K = R // G, TOP * R // n, D // T, D // n
    S = EPG * cap
    W = i1s.shape[2]
    C, Dc = ps.shape[1], ps.shape[4]
    half = EPG // SIDES
    lane, side = i % half, i // half
    others = [(g + 1 + k) % G for k in range(G - 1)]

    def side_for(q, h):
        return (h - q + G) // G

    def relays(h):
        return side == side_for(g, h)

    def outside(h):
        return (SIDES * h) // G

    def origins(h):
        return [(outside(h) + k) % SIDES for k in range(SIDES)]

    outer = side == outside(g)

    barrier = pltpu.get_barrier_semaphore()

    def greet(k, c):
        pl.semaphore_signal(barrier, inc=1, device_id={"fs": (me + k) % n}, device_id_type=MESH)
        return c

    lax.fori_loop(1, n, greet, 0)
    for o in range(1, T):
        pl.semaphore_signal(barrier, inc=1, device_id={"tp": (tpi + o) % T}, device_id_type=MESH)

    loads = [
        pltpu.make_async_copy(src, dst, in_sem.at[k])
        for k, (src, dst) in enumerate(
            ((tokens_in, tokens), (gate_in, w_gate), (up_in, w_up), (down_in, w_down))
        )
    ]
    for load in loads:
        load.start()

    def block(p):
        return pl.ds(pl.multiple_of(p * K, K), K)

    def slots(p):
        return pl.ds(pl.multiple_of(p * cap, cap), cap)

    diagonal = index_grid((K, K), 0) == index_grid((K, K), 1)
    gains = jnp.sum(jnp.where(diagonal, gain[...], 0.0), axis=1, keepdims=True)

    def cast_weights(m, src, scaled):
        def cast(p, c):
            v = src[p]
            wb[m, p] = (v * gains if scaled else v).astype(BF16)
            return c

        loads[1 + m].wait()
        lax.fori_loop(0, n, cast, 0)

    per_part = n // T

    def arrival(m, p):
        return w_rcv.at[m + p // per_part if m == 2 else m]

    def send_weights(m, dst, order):
        for j in order:
            p = partner(me, j, n)
            send(wb.at[m, p], dst.at[block(me)], w_snd.at[m], arrival(m, me), fs=p).start()

    near, far = range(1, EPG), range(EPG, n)

    def blocks(m, dst, p, count):
        rows = dst.at[pl.ds(0, count * K)]
        return send(rows, rows, w_snd.at[m], arrival(m, p), fs=p)

    id0, id1 = ids[0:1, :].astype(F32), ids[1:2, :].astype(F32)
    gap = logit[0:1, :] - logit[1:2, :]
    gid = jnp.floor(id0 * (1.0 / EPG))
    experts = index_grid((n, R), 0)
    m0, m1 = experts == id0, experts == id1
    before = jnp.where(index_grid((R, R), 0) < index_grid((R, R), 1), 1.0, 0.0).astype(BF16)
    rank = dot(jnp.where(m0 | m1, 1.0, 0.0).astype(BF16), before)
    in_group = index_grid((max(G, 16), R), 0) == gid
    group_rank = dot(jnp.where(in_group, 1.0, 0.0).astype(BF16), before)
    slot0 = jnp.sum(jnp.where(m0, rank, 0.0), axis=0, keepdims=True) + (id0 - EPG * gid) * cap
    slot1 = jnp.sum(jnp.where(m1, rank, 0.0), axis=0, keepdims=True) + (id1 - EPG * gid) * cap
    pos = jnp.sum(jnp.where(in_group, group_rank, 0.0), axis=0, keepdims=True)
    line = index_grid((8, R), 0)
    table = jnp.zeros((8, R), F32)
    rows = (slot0, slot1, prob[...] * jax.nn.sigmoid(gap), prob[...] * jax.nn.sigmoid(-gap), gid, pos)
    for at, value in enumerate(rows):
        table = jnp.where(line == at, value, table)
    info_t[...] = table.T

    step = 64

    def norm(b, c):
        rows = pl.ds(pl.multiple_of(b * step, step), step)
        v = tokens[rows, :].astype(F32)
        scale = lax.rsqrt(jnp.mean(v * v, axis=1, keepdims=True) + EPSILON)
        part = tokens[rows, pl.ds(pl.multiple_of(tpi * Dt, Dt), Dt)].astype(F32)
        normed[rows, :] = (part * scale).astype(BF16)
        return c

    loads[0].wait()
    lax.fori_loop(0, R // step, norm, 0)

    def choose(q):
        pick = jnp.where((index_grid((W, R), 0) == pos) & (gid == q.astype(F32)), 1.0, 0.0)
        info_q = dot(table, pick, ((1,), (1,)), precision=lax.Precision.HIGHEST)
        return dot(pick[:Rg].astype(BF16), normed[...]).astype(BF16), info_q

    for q in others:
        s1s[q], i1s[q] = choose(q)
    pl.semaphore_wait(barrier, n - 1 + T - 1)

    def rows_to(q):
        return [
            send(a.at[q], b.at[g, side], snd.at[q], rcv.at[g, side], fs=q * EPG + half * side_for(q, g) + lane)
            for a, b, snd, rcv in ((i1s, i1r, i1_snd, i1_rcv), (s1s, s1r, s1_snd, s1_rcv))
        ]

    def rows_from(h, k):
        return [
            send(a.at[h], b.at[h, k], snd.at[h], rcv.at[h, k], fs=h * EPG)
            for a, b, snd, rcv in ((i1s, i1r, i1_snd, i1_rcv), (s1s, s1r, s1_snd, s1_rcv))
        ]

    def slots_to(h, k, origin, p):
        return send(
            s2s.at[h, k, slots(p)], x.at[tpi, h, slots(origin)], s2_snd.at[h, k], s2_rcv.at[h, origin // half],
            fs=g * EPG + p,
        )

    def dispatch(h, k, origin):
        slot_q = i1r[h, k]
        grid = index_grid((S, Rg), 0)
        spread = (grid == slot_q[0:1, :Rg]) | (grid == slot_q[1:2, :Rg])
        s2s[h, k] = dot(jnp.where(spread, 1.0, 0.0).astype(BF16), s1r[h, k]).astype(BF16)
        for j in range(1, EPG):
            slots_to(h, k, origin, partner(i, j, EPG)).start()
        x[tpi, h, slots(origin), :] = s2s[h, k, slots(i), :]

    def selection(h, k):
        cols = i1r[h, k].T[:Rg]
        grid = index_grid((Rg, S), 1)
        for c in range(TOP):
            sel[h, k, c] = jnp.where(grid == cols[:, c : c + 1], 1.0, 0.0).astype(BF16)

    for q in others:
        for copy in rows_to(q):
            copy.start()
    s1r[g, 0], i1r[g, 0] = choose(g)
    dispatch(g, 0, i)
    cast_weights(0, w_gate, True)
    send_weights(0, new_gate, near)
    cast_weights(1, w_up, True)
    send_weights(1, new_up, near)
    send_weights(0, new_gate, far)
    send_weights(1, new_up, far)
    cast_weights(2, w_down, False)
    for m, dst in enumerate((new_gate, new_up, new_down)):
        dst[block(me), :] = wb[m, me]

    for h in others:

        @pl.when(relays(h))
        def _():
            for k in origins(h):
                for copy in rows_from(h, k):
                    copy.wait_recv()
                dispatch(h, k, k * half + lane)

    send_weights(2, new_down, near)

    @pl.when(jnp.logical_not(outer))
    def _():
        send_weights(2, new_down, [b + j for b in range(EPG, n, EPG) for j in (*range(half, EPG), *range(half))])


    for h in others:

        @pl.when(relays(h))
        def _():
            for k in range(SIDES):
                selection(h, k)

        grid = index_grid((R, Rg), 1)
        here = (grid == info_t[:, 5:6]) & (info_t[:, 4:5] == h.astype(F32))
        place[h] = jnp.where(here, 1.0, 0.0).astype(BF16)
    selection(g, 0)
    grid = index_grid((R, Rg), 1)
    here = (grid == info_t[:, 5:6]) & (info_t[:, 4:5] == g.astype(F32))
    place[g] = jnp.where(here, 1.0, 0.0).astype(BF16)

    part = half * cap

    def portion(k):
        return pl.ds(pl.multiple_of(k * part, part), part)

    def shared(t, h, k, o):
        return send(
            x.at[t, h, portion(k)], x.at[t, h, portion(k)], tp_snd.at[h, k, o - 1], tp_rcv.at[h, k, o - 1],
            tp=(tpi + o) % T,
        )

    def take(ref, snd, rcv, full, count):
        for missing in (0, 1):

            @pl.when(full if missing == 0 else jnp.logical_not(full))
            def _():
                rows = ref.at[pl.ds(0, (count - missing) * cap)]
                send(rows, rows, snd, rcv, fs=me).wait_recv()

    def exchange(h, k, whole):
        take(x.at[tpi, h], s2_snd.at[h, k], s2_rcv.at[h, k], whole, half)
        for o in range(1, T):
            shared(tpi, h, k, o).start()

    def exchanged(h, k):
        for o in range(1, T):
            shared((tpi + T - o) % T, h, k, o).wait_recv()

    def apply_experts(h, k):
        rows = portion(k)
        gate_pre = up_pre = 0.0
        for t in range(T):
            piece = x[t, h, rows, :]
            gate_pre += dot(piece, new_gate[t * Dt : (t + 1) * Dt, :])
            up_pre += dot(piece, new_up[t * Dt : (t + 1) * Dt, :])
        hid[h, rows, :] = (gate_pre / (1.0 + jnp.exp(-gate_pre)) * up_pre).astype(BF16)

    stores = [
        pltpu.make_async_copy(src, dst, out_sem.at[k])
        for k, (src, dst) in enumerate(((new_gate, gate_out), (new_up, up_out), (new_down, down_out)))
    ]
    for k in range(SIDES):
        exchange(g, k, side != k)
    blocks(0, new_gate, me, n - 1).wait_recv()
    stores[0].start()
    for at in range(SIDES):
        for h in others:
            exchange(h, origins(h)[at], jnp.logical_not(relays(h)))
        if at == FAR_AFTER:

            @pl.when(outer)
            def _():
                send_weights(2, new_down, far)

    blocks(1, new_up, me, n - 1).wait_recv()
    stores[1].start()
    for k in range(SIDES):
        exchanged(g, k)
        apply_experts(g, k)
    for at in range(SIDES):
        for h in others:
            exchanged(h, origins(h)[at])
            apply_experts(h, origins(h)[at])

    def partial(h, c, o, t):
        return send(ps.at[o, c, h], pr.at[o, c, h], p_snd.at[0], p_rcv.at[c, h, o - 1], tp=t)

    def sum_units(t, o, c, h):
        rows = pl.ds(pl.multiple_of(t * Dt + c * Dc, Dc), Dc)
        ps[o, c, h] = dot(hid[h], new_down[rows, :], ((1,), (1,))).astype(BF16)

        @pl.when(t != tpi)
        def _():
            partial(h, c, o, t).start()

    def return_to(h, c, k, origin, p, q):
        return send(
            eo.at[c, h, slots(origin)], ret.at[c, h, k, slots(q)], r_snd.at[h], r_rcv.at[c, h, k],
            fs=g * EPG + p,
        )

    def total_units(c, h):
        total = ps[0, c, h].astype(F32)
        for o in range(1, T):
            partial(h, c, o, (tpi + o) % T).wait_recv()
            total += pr[o, c, h].astype(F32)
        eo[c, h] = total.astype(BF16)

    def hand_back_other(c, h):
        total_units(c, h)
        at = half * side_for(g, h)
        for k in range(SIDES):

            @pl.when(relays(h))
            def _():
                ret[c, h, k, slots(i), :] = eo[c, h, slots(k * half + lane), :]

            @pl.when(jnp.logical_not(relays(h)))
            def _():
                return_to(h, c, k, k * half + lane, at + lane, i).start()

            for j in range(1, half):
                l = partner(lane, j, half)
                return_to(h, c, k, k * half + l, at + l, i).start()

    def hand_back_own(c):
        total_units(c, g)
        for j in range(1, EPG):
            p = partner(i, j, EPG)
            return_to(g, c, 0, p, p, i).start()
        ret[c, g, 0, slots(i), :] = eo[c, g, slots(i), :]

    def result_to(h, c, k, q):
        return send(
            ms.at[c, h, k], fin.at[c, q], f_snd.at[h, k], f_rcv.at[c, q], fs=h * EPG + k * half + lane
        )

    def mix(c, h, k):
        rows = ret.at[c, h, k, pl.ds(0, (EPG - 1) * cap)]
        send(rows, rows, r_snd.at[h], r_rcv.at[c, h, k], fs=me).wait_recv()
        cols = i1r[h, k].T[:Rg]
        outs = ret[c, h, k]
        return (cols[:, 2:3] * dot(sel[h, k, 0], outs) + cols[:, 3:4] * dot(sel[h, k, 1], outs)).astype(BF16)

    def mix_other(c, h):
        @pl.when(relays(h))
        def _():
            for k in range(SIDES):
                ms[c, h, k] = mix(c, h, k)
                result_to(h, c, k, g).start()

    first = me // per_part
    for k in range(T):
        t = (first + k) % T
        if k == 0:
            blocks(2, new_down, me, per_part - 1).wait_recv()
        else:
            blocks(2, new_down, t * per_part, per_part).wait_recv()
        if k == T - 1:
            stores[2].start()
        for h in others:
            for c in range(C):
                sum_units(t, (t - tpi + T) % T, c, h)

        @pl.when(t == tpi)
        def _():
            for h in others:
                for c in range(C):
                    hand_back_other(c, h)

        for c in range(C):
            sum_units(t, (t - tpi + T) % T, c, g)

        @pl.when(t == tpi)
        def _():
            for c in range(C):
                hand_back_own(c)


    for h in others:
        for c in range(C):
            mix_other(c, h)

    for c in range(C):
        fin[c, g] = mix(c, g, 0)

    for c in range(C):
        total = 0.0
        for k in (G - 1, *range(G - 1)):
            q = (g + 1 + k) % G
            if k < G - 1:
                result_to(q, c, 0, q).wait_recv()
            total += dot(place[q], fin[c, q])
        mixed[:, c * Dc : (c + 1) * Dc] = total.astype(BF16)
        stores.append(
            pltpu.make_async_copy(
                mixed.at[:, c * Dc : (c + 1) * Dc], mixed_out.at[:, c * Dc : (c + 1) * Dc], out_sem.at[3 + c]
            )
        )
        stores[-1].start()
    for store in stores:
        store.wait()

    def drain(ref, sem):
        send(ref, ref, sem, sem, fs=me).wait_send()

    for m in range(3):
        drain(wb.at[m, pl.ds(0, n - 1)], w_snd.at[m])
    sent = pl.ds(0, (EPG - 1) * cap)
    drain(s2s.at[g, 0, sent], s2_snd.at[g, 0])
    drain(eo.at[pl.ds(0, C), g, sent], r_snd.at[g])
    if T > 1:
        drain(ps.at[pl.ds(1, T - 1)], p_snd.at[0])
    for h in (*others, g):
        for k in range(SIDES):
            for o in range(1, T):
                shared(tpi, h, k, o).wait_send()
    for h in others:
        for copy in rows_to(h):
            copy.wait_send()

        @pl.when(relays(h))
        def _():
            drain(eo.at[pl.ds(0, C), h, pl.ds(0, (EPG - SIDES) * cap)], r_snd.at[h])
            for k in range(SIDES):
                drain(s2s.at[h, k, sent], s2_snd.at[h, k])
                drain(ms.at[pl.ds(0, C), h, k], f_snd.at[h, k])

        @pl.when(jnp.logical_not(relays(h)))
        def _():
            drain(eo.at[pl.ds(0, C), h], r_snd.at[h])


def hand_over(count, *refs):
    sources, results, rooms = refs[:4], refs[4:8], refs[8:12]
    arrived, left = refs[12:]
    into, out = [], []
    for a, (source, room, result) in enumerate(zip(sources, rooms, results)):
        height = source.shape[0] // count
        for b in range(count):
            rows = pl.ds(b * height, height)
            into.append(pltpu.make_async_copy(source.at[rows], room.at[rows], arrived.at[a, b]))
            out.append(pltpu.make_async_copy(room.at[rows], result.at[rows], left.at[a, b]))
    for copy in into:
        copy.start()
    for first, second in zip(into, out):
        first.wait()
        second.start()
    for copy in out:
        copy.wait()


def local(tokens, norm_gain, w_gate, w_up, w_down, route_expert, group_prob, pair_logit):
    n, T = lax.axis_size("fs"), lax.axis_size("tp")
    R, D = tokens.shape
    F = w_gate.shape[2]
    G = n // EPG
    Rg, cap, Dt = R // G, TOP * R // n, D // T
    S, W = EPG * cap, max(Rg, 128)
    Dc = min(Dt, max(Dt // CHUNKS, 128))
    C = Dt // Dc
    vmem = pl.BlockSpec(memory_space=pltpu.VMEM)
    hbm = pl.BlockSpec(memory_space=pl.ANY)
    sem = pltpu.SemaphoreType.DMA
    weights = jax.ShapeDtypeStruct((D, F), BF16)
    shapes = [weights, weights, weights, jax.ShapeDtypeStruct((R, Dt), BF16)]
    results = pl.pallas_call(
        functools.partial(kernel, n, T),
        out_shape=shapes,
        in_specs=[vmem] * 4 + [hbm] * 4,
        out_specs=[hbm] * 4,
        scratch_shapes=[
            pltpu.VMEM((R, D), BF16),
            pltpu.VMEM(w_gate.shape, F32),
            pltpu.VMEM(w_up.shape, F32),
            pltpu.VMEM(w_down.shape, F32),
            pltpu.VMEM((D, F), BF16),
            pltpu.VMEM((D, F), BF16),
            pltpu.VMEM((D, F), BF16),
            pltpu.VMEM((R, Dt), BF16),
            pltpu.VMEM((3, n, D // n, F), BF16),
            pltpu.VMEM((R, Dt), BF16),
            pltpu.VMEM((R, 8), F32),
            pltpu.VMEM((G, Rg, Dt), BF16),
            pltpu.VMEM((G, 8, W), F32),
            pltpu.VMEM((G, SIDES, Rg, Dt), BF16),
            pltpu.VMEM((G, SIDES, 8, W), F32),
            pltpu.VMEM((G, SIDES, S, Dt), BF16),
            pltpu.VMEM((T, G, S, Dt), BF16),
            pltpu.VMEM((G, SIDES, TOP, Rg, S), BF16),
            pltpu.VMEM((G, R, Rg), BF16),
            pltpu.VMEM((G, S, F), BF16),
            pltpu.VMEM((T, C, G, S, Dc), BF16),
            pltpu.VMEM((T, C, G, S, Dc), BF16),
            pltpu.VMEM((C, G, S, Dc), BF16),
            pltpu.VMEM((C, G, SIDES, S, Dc), BF16),
            pltpu.VMEM((C, G, SIDES, Rg, Dc), BF16),
            pltpu.VMEM((C, G, Rg, Dc), BF16),
            sem((4,)), sem((3 + C,)),
            sem((3,)), sem((2 + T,)),
            sem((G,)), sem((G, SIDES)), sem((G,)), sem((G, SIDES)),
            sem((G, SIDES)), sem((G, SIDES)),
            sem((G, SIDES, max(T - 1, 1))), sem((G, SIDES, max(T - 1, 1))), sem((1,)), sem((C, G, max(T - 1, 1))),
            sem((G,)), sem((C, G, SIDES)),
            sem((G, SIDES)), sem((C, G)),
        ],
        compiler_params=pltpu.CompilerParams(
            collective_id=0, has_side_effects=True, vmem_limit_bytes=VMEM_LIMIT
        ),
    )(
        route_expert.T, norm_gain[None, :], group_prob[None, :], pair_logit.T,
        tokens, w_gate, w_up, w_down,
    )
    parts = 2
    gate, up, down, mixed = pl.pallas_call(
        functools.partial(hand_over, parts),
        out_shape=shapes,
        in_specs=[hbm] * 4,
        out_specs=[hbm] * 4,
        scratch_shapes=[pltpu.VMEM(s.shape, s.dtype) for s in shapes] + [sem((4, parts)), sem((4, parts))],
    )(*results)
    return gate[None], up[None], down[None], mixed


def solution(mesh):
    placed = (
        P("fs", None),
        P("fs"),
        P(None, "fs", "tp"),
        P(None, "fs", "tp"),
        P(None, "fs", "tp"),
        P("fs", None),
        P("fs"),
        P("fs", None),
    )
    return jax.shard_map(
        local,
        mesh=mesh,
        in_specs=placed,
        out_specs=(P("fs", None, "tp"), P("fs", None, "tp"), P("fs", None, "tp"), P("fs", "tp")),
        check_vma=False,
    )
```

```python
import functools

import jax
import jax.numpy as jnp
from jax import lax
from jax.experimental import pallas as pl
from jax.experimental.pallas import tpu as pltpu
from jax.sharding import PartitionSpec as P

EPG = 8
SIDES = 2
TOP = 2
EPSILON = 1e-06
MESH = pl.DeviceIdType.MESH
F32, BF16 = jnp.float32, jnp.bfloat16
CHUNKS = 4
FAR_AFTER = 1
VMEM_LIMIT = 62 * 1024 * 1024


def index_grid(shape, dim):
    return lax.broadcasted_iota(jnp.int32, shape, dim).astype(F32)


def dot(a, b, contract=((1,), (0,)), **kw):
    return lax.dot_general(a, b, (contract, ((), ())), preferred_element_type=F32, **kw)


def send(src, dst, send_sem, recv_sem, **where):
    return pltpu.make_async_remote_copy(
        src_ref=src, dst_ref=dst, send_sem=send_sem, recv_sem=recv_sem, device_id=where, device_id_type=MESH
    )


def partner(me, j, n):
    if n & (n - 1):
        return (me + j) % n
    p, bit = 0, 1
    while bit < n:
        here = (me // bit) % 2
        p = p + bit * (1 - here if j & bit else here)
        bit *= 2
    return p


def kernel(
    n, T, ids_in, gain_in, prob_in, logit_in, tokens_in, gate_in, up_in, down_in, gate_out, up_out, down_out, mixed_out,
    ids, gain, prob, logit, tokens, w_gate, w_up, w_down, new_gate, new_up, new_down, mixed,
    wb, normed, info_t, s1s, i1s, s1r, i1r, s2s, x, sel, place, hid, ps, pr, eo, ret, ms, fin,
    in_sem, out_sem, w_snd, w_rcv, s1_snd, s1_rcv, i1_snd, i1_rcv, s2_snd, s2_rcv, tp_snd, tp_rcv,
    p_snd, p_rcv, r_snd, r_rcv, f_snd, f_rcv,
):
    me, tpi = lax.axis_index("fs"), lax.axis_index("tp")
    R, D = tokens.shape
    G = n // EPG
    g, i = me // EPG, me % EPG
    Rg, cap, Dt, K = R // G, TOP * R // n, D // T, D // n
    S = EPG * cap
    W = i1s.shape[2]
    C, Dc = ps.shape[1], ps.shape[4]
    half = EPG // SIDES
    lane, side = i % half, i // half
    others = [(g + 1 + k) % G for k in range(G - 1)]

    def side_for(q, h):
        return (h - q + G) // G

    def relays(h):
        return side == side_for(g, h)

    def outside(h):
        return (SIDES * h) // G

    def origins(h):
        return [(outside(h) + k) % SIDES for k in range(SIDES)]

    outer = side == outside(g)

    barrier = pltpu.get_barrier_semaphore()

    loads = [
        pltpu.make_async_copy(src, dst, in_sem.at[k])
        for k, (src, dst) in enumerate(
            (
                (gate_in, w_gate), (up_in, w_up), (down_in, w_down), (tokens_in, tokens),
                (ids_in, ids), (logit_in, logit), (prob_in, prob), (gain_in, gain),
            )
        )
    ]
    for k in (4, 5, 6, 3, 7, 0, 1, 2):
        loads[k].start()

    def greet(k, c):
        pl.semaphore_signal(barrier, inc=1, device_id={"fs": (me + k) % n}, device_id_type=MESH)
        return c

    lax.fori_loop(1, n, greet, 0)
    for o in range(1, T):
        pl.semaphore_signal(barrier, inc=1, device_id={"tp": (tpi + o) % T}, device_id_type=MESH)

    def block(p):
        return pl.ds(pl.multiple_of(p * K, K), K)

    def slots(p):
        return pl.ds(pl.multiple_of(p * cap, cap), cap)

    def spread_gain():
        diagonal = index_grid((K, K), 0) == index_grid((K, K), 1)
        return jnp.sum(jnp.where(diagonal, gain[...], 0.0), axis=1, keepdims=True)

    def cast_weights(m, src, scaled):
        gains = spread_gain() if scaled else None

        def cast(p, c):
            v = src[p]
            wb[m, p] = (v * gains if scaled else v).astype(BF16)
            return c

        loads[m].wait()
        lax.fori_loop(0, n, cast, 0)

    per_part = n // T

    def arrival(m, p):
        return w_rcv.at[m + p // per_part if m == 2 else m]

    def send_weights(m, dst, order):
        for j in order:
            p = partner(me, j, n)
            send(wb.at[m, p], dst.at[block(me)], w_snd.at[m], arrival(m, me), fs=p).start()

    near, far = range(1, EPG), range(EPG, n)

    def blocks(m, dst, p, count):
        rows = dst.at[pl.ds(0, count * K)]
        return send(rows, rows, w_snd.at[m], arrival(m, p), fs=p)

    for k in (4, 5, 6):
        loads[k].wait()
    id0, id1 = ids[0:1, :].astype(F32), ids[1:2, :].astype(F32)
    gap = logit[0:1, :] - logit[1:2, :]
    gid = jnp.floor(id0 * (1.0 / EPG))
    experts = index_grid((n, R), 0)
    m0, m1 = experts == id0, experts == id1
    before = jnp.where(index_grid((R, R), 0) < index_grid((R, R), 1), 1.0, 0.0).astype(BF16)
    rank = dot(jnp.where(m0 | m1, 1.0, 0.0).astype(BF16), before)
    in_group = index_grid((max(G, 16), R), 0) == gid
    group_rank = dot(jnp.where(in_group, 1.0, 0.0).astype(BF16), before)
    slot0 = jnp.sum(jnp.where(m0, rank, 0.0), axis=0, keepdims=True) + (id0 - EPG * gid) * cap
    slot1 = jnp.sum(jnp.where(m1, rank, 0.0), axis=0, keepdims=True) + (id1 - EPG * gid) * cap
    pos = jnp.sum(jnp.where(in_group, group_rank, 0.0), axis=0, keepdims=True)
    line = index_grid((8, R), 0)
    table = jnp.zeros((8, R), F32)
    rows = (slot0, slot1, prob[...] * jax.nn.sigmoid(gap), prob[...] * jax.nn.sigmoid(-gap), gid, pos)
    for at, value in enumerate(rows):
        table = jnp.where(line == at, value, table)
    info_t[...] = table.T

    step = 64

    def norm(b, c):
        rows = pl.ds(pl.multiple_of(b * step, step), step)
        v = tokens[rows, :].astype(F32)
        scale = lax.rsqrt(jnp.mean(v * v, axis=1, keepdims=True) + EPSILON)
        part = tokens[rows, pl.ds(pl.multiple_of(tpi * Dt, Dt), Dt)].astype(F32)
        normed[rows, :] = (part * scale).astype(BF16)
        return c

    loads[3].wait()
    lax.fori_loop(0, R // step, norm, 0)

    def choose(q):
        pick = jnp.where((index_grid((W, R), 0) == pos) & (gid == q.astype(F32)), 1.0, 0.0)
        info_q = dot(table, pick, ((1,), (1,)), precision=lax.Precision.HIGHEST)
        return dot(pick[:Rg].astype(BF16), normed[...]).astype(BF16), info_q

    for q in others:
        s1s[q], i1s[q] = choose(q)
    pl.semaphore_wait(barrier, n - 1 + T - 1)

    def rows_to(q):
        return [
            send(a.at[q], b.at[g, side], snd.at[q], rcv.at[g, side], fs=q * EPG + half * side_for(q, g) + lane)
            for a, b, snd, rcv in ((i1s, i1r, i1_snd, i1_rcv), (s1s, s1r, s1_snd, s1_rcv))
        ]

    def rows_from(h, k):
        return [
            send(a.at[h], b.at[h, k], snd.at[h], rcv.at[h, k], fs=h * EPG)
            for a, b, snd, rcv in ((i1s, i1r, i1_snd, i1_rcv), (s1s, s1r, s1_snd, s1_rcv))
        ]

    def slots_to(h, k, origin, p):
        return send(
            s2s.at[h, k, slots(p)], x.at[tpi, h, slots(origin)], s2_snd.at[h, k], s2_rcv.at[h, origin // half],
            fs=g * EPG + p,
        )

    def dispatch(h, k, origin):
        slot_q = i1r[h, k]
        grid = index_grid((S, Rg), 0)
        spread = (grid == slot_q[0:1, :Rg]) | (grid == slot_q[1:2, :Rg])
        s2s[h, k] = dot(jnp.where(spread, 1.0, 0.0).astype(BF16), s1r[h, k]).astype(BF16)
        for j in range(1, EPG):
            slots_to(h, k, origin, partner(i, j, EPG)).start()
        x[tpi, h, slots(origin), :] = s2s[h, k, slots(i), :]

    def selection(h, k):
        cols = i1r[h, k].T[:Rg]
        grid = index_grid((Rg, S), 1)
        for c in range(TOP):
            sel[h, k, c] = jnp.where(grid == cols[:, c : c + 1], 1.0, 0.0).astype(BF16)

    for q in others:
        for copy in rows_to(q):
            copy.start()
    s1r[g, 0], i1r[g, 0] = choose(g)
    loads[7].wait()
    dispatch(g, 0, i)
    cast_weights(0, w_gate, True)
    send_weights(0, new_gate, near)
    cast_weights(1, w_up, True)
    send_weights(1, new_up, near)
    send_weights(0, new_gate, far)
    send_weights(1, new_up, far)
    cast_weights(2, w_down, False)
    for m, dst in enumerate((new_gate, new_up, new_down)):
        dst[block(me), :] = wb[m, me]

    for h in others:

        @pl.when(relays(h))
        def _():
            for k in origins(h):
                for copy in rows_from(h, k):
                    copy.wait_recv()
                dispatch(h, k, k * half + lane)

    send_weights(2, new_down, near)

    @pl.when(jnp.logical_not(outer))
    def _():
        send_weights(2, new_down, [b + j for b in range(EPG, n, EPG) for j in (*range(half, EPG), *range(half))])


    for h in others:

        @pl.when(relays(h))
        def _():
            for k in range(SIDES):
                selection(h, k)

        grid = index_grid((R, Rg), 1)
        here = (grid == info_t[:, 5:6]) & (info_t[:, 4:5] == h.astype(F32))
        place[h] = jnp.where(here, 1.0, 0.0).astype(BF16)
    selection(g, 0)
    grid = index_grid((R, Rg), 1)
    here = (grid == info_t[:, 5:6]) & (info_t[:, 4:5] == g.astype(F32))
    place[g] = jnp.where(here, 1.0, 0.0).astype(BF16)

    part = half * cap

    def portion(k):
        return pl.ds(pl.multiple_of(k * part, part), part)

    def shared(t, h, k, o):
        return send(
            x.at[t, h, portion(k)], x.at[t, h, portion(k)], tp_snd.at[h, k, o - 1], tp_rcv.at[h, k, o - 1],
            tp=(tpi + o) % T,
        )

    def take(ref, snd, rcv, full, count):
        for missing in (0, 1):

            @pl.when(full if missing == 0 else jnp.logical_not(full))
            def _():
                rows = ref.at[pl.ds(0, (count - missing) * cap)]
                send(rows, rows, snd, rcv, fs=me).wait_recv()

    def exchange(h, k, whole):
        take(x.at[tpi, h], s2_snd.at[h, k], s2_rcv.at[h, k], whole, half)
        for o in range(1, T):
            shared(tpi, h, k, o).start()

    def exchanged(h, k):
        for o in range(1, T):
            shared((tpi + T - o) % T, h, k, o).wait_recv()

    def apply_experts(h, k):
        rows = portion(k)
        gate_pre = up_pre = 0.0
        for t in range(T):
            piece = x[t, h, rows, :]
            gate_pre += dot(piece, new_gate[t * Dt : (t + 1) * Dt, :])
            up_pre += dot(piece, new_up[t * Dt : (t + 1) * Dt, :])
        hid[h, rows, :] = (gate_pre / (1.0 + jnp.exp(-gate_pre)) * up_pre).astype(BF16)

    stores = [
        pltpu.make_async_copy(src, dst, out_sem.at[k])
        for k, (src, dst) in enumerate(((new_gate, gate_out), (new_up, up_out), (new_down, down_out)))
    ]
    for k in range(SIDES):
        exchange(g, k, side != k)
    blocks(0, new_gate, me, n - 1).wait_recv()
    stores[0].start()
    for at in range(SIDES):
        for h in others:
            exchange(h, origins(h)[at], jnp.logical_not(relays(h)))
        if at == FAR_AFTER:

            @pl.when(outer)
            def _():
                send_weights(2, new_down, far)

    blocks(1, new_up, me, n - 1).wait_recv()
    stores[1].start()
    for k in range(SIDES):
        exchanged(g, k)
        apply_experts(g, k)
    for at in range(SIDES):
        for h in others:
            exchanged(h, origins(h)[at])
            apply_experts(h, origins(h)[at])

    def partial(h, c, o, t):
        return send(ps.at[o, c, h], pr.at[o, c, h], p_snd.at[0], p_rcv.at[c, h, o - 1], tp=t)

    def sum_units(t, o, c, h):
        rows = pl.ds(pl.multiple_of(t * Dt + c * Dc, Dc), Dc)
        ps[o, c, h] = dot(hid[h], new_down[rows, :], ((1,), (1,))).astype(BF16)

        @pl.when(t != tpi)
        def _():
            partial(h, c, o, t).start()

    def return_to(h, c, k, origin, p, q):
        return send(
            eo.at[c, h, slots(origin)], ret.at[c, h, k, slots(q)], r_snd.at[h], r_rcv.at[c, h, k],
            fs=g * EPG + p,
        )

    def total_units(c, h):
        total = ps[0, c, h].astype(F32)
        for o in range(1, T):
            partial(h, c, o, (tpi + o) % T).wait_recv()
            total += pr[o, c, h].astype(F32)
        eo[c, h] = total.astype(BF16)

    def hand_back_other(c, h):
        total_units(c, h)
        at = half * side_for(g, h)
        for k in range(SIDES):

            @pl.when(relays(h))
            def _():
                ret[c, h, k, slots(i), :] = eo[c, h, slots(k * half + lane), :]

            @pl.when(jnp.logical_not(relays(h)))
            def _():
                return_to(h, c, k, k * half + lane, at + lane, i).start()

            for j in range(1, half):
                l = partner(lane, j, half)
                return_to(h, c, k, k * half + l, at + l, i).start()

    def hand_back_own(c):
        total_units(c, g)
        for j in range(1, EPG):
            p = partner(i, j, EPG)
            return_to(g, c, 0, p, p, i).start()
        ret[c, g, 0, slots(i), :] = eo[c, g, slots(i), :]

    def result_to(h, c, k, q):
        return send(
            ms.at[c, h, k], fin.at[c, q], f_snd.at[h, k], f_rcv.at[c, q], fs=h * EPG + k * half + lane
        )

    def mix(c, h, k):
        rows = ret.at[c, h, k, pl.ds(0, (EPG - 1) * cap)]
        send(rows, rows, r_snd.at[h], r_rcv.at[c, h, k], fs=me).wait_recv()
        cols = i1r[h, k].T[:Rg]
        outs = ret[c, h, k]
        return (cols[:, 2:3] * dot(sel[h, k, 0], outs) + cols[:, 3:4] * dot(sel[h, k, 1], outs)).astype(BF16)

    def mix_other(c, h):
        @pl.when(relays(h))
        def _():
            for k in range(SIDES):
                ms[c, h, k] = mix(c, h, k)
                result_to(h, c, k, g).start()

    first = me // per_part
    for k in range(T):
        t = (first + k) % T
        if k == 0:
            blocks(2, new_down, me, per_part - 1).wait_recv()
        else:
            blocks(2, new_down, t * per_part, per_part).wait_recv()
        if k == T - 1:
            stores[2].start()
        for h in others:
            for c in range(C):
                sum_units(t, (t - tpi + T) % T, c, h)

        @pl.when(t == tpi)
        def _():
            for h in others:
                for c in range(C):
                    hand_back_other(c, h)

        for c in range(C):
            sum_units(t, (t - tpi + T) % T, c, g)

        @pl.when(t == tpi)
        def _():
            for c in range(C):
                hand_back_own(c)


    for h in others:
        for c in range(C):
            mix_other(c, h)

    for c in range(C):
        fin[c, g] = mix(c, g, 0)
        total = dot(place[g], fin[c, g])
        for q in others:
            result_to(q, c, 0, q).wait_recv()
            total += dot(place[q], fin[c, q])
        mixed[:, c * Dc : (c + 1) * Dc] = total.astype(BF16)
        stores.append(
            pltpu.make_async_copy(
                mixed.at[:, c * Dc : (c + 1) * Dc], mixed_out.at[:, c * Dc : (c + 1) * Dc], out_sem.at[3 + c]
            )
        )
        stores[-1].start()
    for store in stores:
        store.wait()

    def drain(ref, sem):
        send(ref, ref, sem, sem, fs=me).wait_send()

    for m in range(3):
        drain(wb.at[m, pl.ds(0, n - 1)], w_snd.at[m])
    sent = pl.ds(0, (EPG - 1) * cap)
    drain(s2s.at[g, 0, sent], s2_snd.at[g, 0])
    drain(eo.at[pl.ds(0, C), g, sent], r_snd.at[g])
    if T > 1:
        drain(ps.at[pl.ds(1, T - 1)], p_snd.at[0])
    for h in (*others, g):
        for k in range(SIDES):
            for o in range(1, T):
                shared(tpi, h, k, o).wait_send()
    for h in others:
        for copy in rows_to(h):
            copy.wait_send()

        @pl.when(relays(h))
        def _():
            drain(eo.at[pl.ds(0, C), h, pl.ds(0, (EPG - SIDES) * cap)], r_snd.at[h])
            for k in range(SIDES):
                drain(s2s.at[h, k, sent], s2_snd.at[h, k])
                drain(ms.at[pl.ds(0, C), h, k], f_snd.at[h, k])

        @pl.when(jnp.logical_not(relays(h)))
        def _():
            drain(eo.at[pl.ds(0, C), h], r_snd.at[h])


def hand_over(count, *refs):
    sources, results, rooms = refs[:4], refs[4:8], refs[8:12]
    arrived, left = refs[12:]
    into, out = [], []
    for a, (source, room, result) in enumerate(zip(sources, rooms, results)):
        height = source.shape[0] // count
        for b in range(count):
            rows = pl.ds(b * height, height)
            into.append(pltpu.make_async_copy(source.at[rows], room.at[rows], arrived.at[a, b]))
            out.append(pltpu.make_async_copy(room.at[rows], result.at[rows], left.at[a, b]))
    for copy in into:
        copy.start()
    for first, second in zip(into, out):
        first.wait()
        second.start()
    for copy in out:
        copy.wait()


def local(tokens, norm_gain, w_gate, w_up, w_down, route_expert, group_prob, pair_logit):
    n, T = lax.axis_size("fs"), lax.axis_size("tp")
    R, D = tokens.shape
    F = w_gate.shape[2]
    G = n // EPG
    Rg, cap, Dt = R // G, TOP * R // n, D // T
    S, W = EPG * cap, max(Rg, 128)
    Dc = min(Dt, max(Dt // CHUNKS, 128))
    C = Dt // Dc
    hbm = pl.BlockSpec(memory_space=pl.ANY)
    sem = pltpu.SemaphoreType.DMA
    weights = jax.ShapeDtypeStruct((D, F), BF16)
    shapes = [weights, weights, weights, jax.ShapeDtypeStruct((R, Dt), BF16)]
    results = pl.pallas_call(
        functools.partial(kernel, n, T),
        out_shape=shapes,
        in_specs=[hbm] * 8,
        out_specs=[hbm] * 4,
        scratch_shapes=[
            pltpu.VMEM((TOP, R), jnp.int32),
            pltpu.VMEM((1, D // n), F32),
            pltpu.VMEM((1, R), F32),
            pltpu.VMEM((TOP, R), F32),
            pltpu.VMEM((R, D), BF16),
            pltpu.VMEM(w_gate.shape, F32),
            pltpu.VMEM(w_up.shape, F32),
            pltpu.VMEM(w_down.shape, F32),
            pltpu.VMEM((D, F), BF16),
            pltpu.VMEM((D, F), BF16),
            pltpu.VMEM((D, F), BF16),
            pltpu.VMEM((R, Dt), BF16),
            pltpu.VMEM((3, n, D // n, F), BF16),
            pltpu.VMEM((R, Dt), BF16),
            pltpu.VMEM((R, 8), F32),
            pltpu.VMEM((G, Rg, Dt), BF16),
            pltpu.VMEM((G, 8, W), F32),
            pltpu.VMEM((G, SIDES, Rg, Dt), BF16),
            pltpu.VMEM((G, SIDES, 8, W), F32),
            pltpu.VMEM((G, SIDES, S, Dt), BF16),
            pltpu.VMEM((T, G, S, Dt), BF16),
            pltpu.VMEM((G, SIDES, TOP, Rg, S), BF16),
            pltpu.VMEM((G, R, Rg), BF16),
            pltpu.VMEM((G, S, F), BF16),
            pltpu.VMEM((T, C, G, S, Dc), BF16),
            pltpu.VMEM((T, C, G, S, Dc), BF16),
            pltpu.VMEM((C, G, S, Dc), BF16),
            pltpu.VMEM((C, G, SIDES, S, Dc), BF16),
            pltpu.VMEM((C, G, SIDES, Rg, Dc), BF16),
            pltpu.VMEM((C, G, Rg, Dc), BF16),
            sem((8,)), sem((3 + C,)),
            sem((3,)), sem((2 + T,)),
            sem((G,)), sem((G, SIDES)), sem((G,)), sem((G, SIDES)),
            sem((G, SIDES)), sem((G, SIDES)),
            sem((G, SIDES, max(T - 1, 1))), sem((G, SIDES, max(T - 1, 1))), sem((1,)), sem((C, G, max(T - 1, 1))),
            sem((G,)), sem((C, G, SIDES)),
            sem((G, SIDES)), sem((C, G)),
        ],
        compiler_params=pltpu.CompilerParams(
            collective_id=0, has_side_effects=True, vmem_limit_bytes=VMEM_LIMIT
        ),
    )(
        route_expert.T, norm_gain[None, :], group_prob[None, :], pair_logit.T,
        tokens, w_gate, w_up, w_down,
    )
    parts = 2
    gate, up, down, mixed = pl.pallas_call(
        functools.partial(hand_over, parts),
        out_shape=shapes,
        in_specs=[hbm] * 4,
        out_specs=[hbm] * 4,
        scratch_shapes=[pltpu.VMEM(s.shape, s.dtype) for s in shapes] + [sem((4, parts)), sem((4, parts))],
    )(*results)
    return gate[None], up[None], down[None], mixed


def solution(mesh):
    placed = (
        P("fs", None),
        P("fs"),
        P(None, "fs", "tp"),
        P(None, "fs", "tp"),
        P(None, "fs", "tp"),
        P("fs", None),
        P("fs"),
        P("fs", None),
    )
    return jax.shard_map(
        local,
        mesh=mesh,
        in_specs=placed,
        out_specs=(P("fs", None, "tp"), P("fs", None, "tp"), P("fs", None, "tp"), P("fs", "tp")),
        check_vma=False,
    )
```

```python
import functools

import jax
import jax.numpy as jnp
from jax import lax
from jax.experimental import pallas as pl
from jax.experimental.pallas import tpu as pltpu
from jax.sharding import PartitionSpec as P

EPG = 8
SIDES = 2
TOP = 2
EPSILON = 1e-06
MESH = pl.DeviceIdType.MESH
F32, BF16 = jnp.float32, jnp.bfloat16
CHUNKS = 4
STRIPS = 4
VMEM_LIMIT = 62 * 1024 * 1024


def index_grid(shape, dim):
    return lax.broadcasted_iota(jnp.int32, shape, dim).astype(F32)


def dot(a, b, contract=((1,), (0,)), **kw):
    return lax.dot_general(a, b, (contract, ((), ())), preferred_element_type=F32, **kw)


def send(src, dst, send_sem, recv_sem, **where):
    return pltpu.make_async_remote_copy(
        src_ref=src, dst_ref=dst, send_sem=send_sem, recv_sem=recv_sem, device_id=where, device_id_type=MESH
    )


def partner(me, j, n):
    if n & (n - 1):
        return (me + j) % n
    p, bit = 0, 1
    while bit < n:
        here = (me // bit) % 2
        p = p + bit * (1 - here if j & bit else here)
        bit *= 2
    return p


def kernel(
    n, T, ids_in, gain_in, prob_in, logit_in, tokens_in, gate_in, up_in, down_in, gate_out, up_out, down_out, mixed_out,
    ids, gain, prob, logit, tokens, w_gate, w_up, w_down, new_gate, new_up, new_down, mixed,
    wb, normed, info_t, s1s, i1s, s1r, i1r, s2s, x, sel, place, hid, ps, pr, eo, ret, ms, fin,
    in_sem, out_sem, w_snd, w_rcv, s1_snd, s1_rcv, i1_snd, i1_rcv, s2_snd, s2_rcv, tp_snd, tp_rcv,
    p_snd, p_rcv, r_snd, r_rcv, f_snd, f_rcv,
):
    me, tpi = lax.axis_index("fs"), lax.axis_index("tp")
    R, D = tokens.shape
    G = n // EPG
    g, i = me // EPG, me % EPG
    Rg, cap, Dt, K = R // G, TOP * R // n, D // T, D // n
    S = EPG * cap
    W = i1s.shape[2]
    C, Dc = ps.shape[1], ps.shape[4]
    half = EPG // SIDES
    lane, side = i % half, i // half
    others = [(g + 1 + k) % G for k in range(G - 1)]

    def side_for(q, h):
        return (h - q + G) // G

    def relays(h):
        return side == side_for(g, h)

    def outside(h):
        return (SIDES * h) // G

    def origins(h):
        return [(outside(h) + k) % SIDES for k in range(SIDES)]

    outer = side == outside(g)

    barrier = pltpu.get_barrier_semaphore()

    step = min(R, 64)
    strip = max(R // STRIPS, step)
    strips = [pl.ds(k * strip, strip) for k in range(R // strip)]
    loads = [
        pltpu.make_async_copy(src, dst, in_sem.at[k])
        for k, (src, dst) in enumerate(
            (
                (gate_in, w_gate), (up_in, w_up), (down_in, w_down),
                (ids_in, ids), (logit_in, logit), (prob_in, prob), (gain_in, gain),
                *((tokens_in.at[rows], tokens.at[rows]) for rows in strips),
            )
        )
    ]
    for load in loads[3:]:
        load.start()

    def greet(k, c):
        pl.semaphore_signal(barrier, inc=1, device_id={"fs": (me + k) % n}, device_id_type=MESH)
        return c

    lax.fori_loop(1, n, greet, 0)
    for o in range(1, T):
        pl.semaphore_signal(barrier, inc=1, device_id={"tp": (tpi + o) % T}, device_id_type=MESH)

    def block(p):
        return pl.ds(pl.multiple_of(p * K, K), K)

    def slots(p):
        return pl.ds(pl.multiple_of(p * cap, cap), cap)

    def spread_gain():
        diagonal = index_grid((K, K), 0) == index_grid((K, K), 1)
        return jnp.sum(jnp.where(diagonal, gain[...], 0.0), axis=1, keepdims=True)

    def cast_weights(m, src, scaled):
        gains = spread_gain() if scaled else None

        def cast(p, c):
            v = src[p]
            wb[m, p] = (v * gains if scaled else v).astype(BF16)
            return c

        loads[m].wait()
        lax.fori_loop(0, n, cast, 0)

    per_part = n // T

    def arrival(m, p):
        return w_rcv.at[m + p // per_part if m == 2 else m]

    def send_weights(m, dst, order):
        for j in order:
            p = partner(me, j, n)
            send(wb.at[m, p], dst.at[block(me)], w_snd.at[m], arrival(m, me), fs=p).start()

    near, far = range(1, EPG), range(EPG, n)

    def blocks(m, dst, p, count):
        rows = dst.at[pl.ds(0, count * K)]
        return send(rows, rows, w_snd.at[m], arrival(m, p), fs=p)

    for load in loads[3:6]:
        load.wait()
    id0, id1 = ids[0:1, :].astype(F32), ids[1:2, :].astype(F32)
    gap = logit[0:1, :] - logit[1:2, :]
    gid = jnp.floor(id0 * (1.0 / EPG))
    experts = index_grid((n, R), 0)
    m0, m1 = experts == id0, experts == id1
    before = jnp.where(index_grid((R, R), 0) < index_grid((R, R), 1), 1.0, 0.0).astype(BF16)
    rank = dot(jnp.where(m0 | m1, 1.0, 0.0).astype(BF16), before)
    in_group = index_grid((max(G, 16), R), 0) == gid
    group_rank = dot(jnp.where(in_group, 1.0, 0.0).astype(BF16), before)
    slot0 = jnp.sum(jnp.where(m0, rank, 0.0), axis=0, keepdims=True) + (id0 - EPG * gid) * cap
    slot1 = jnp.sum(jnp.where(m1, rank, 0.0), axis=0, keepdims=True) + (id1 - EPG * gid) * cap
    pos = jnp.sum(jnp.where(in_group, group_rank, 0.0), axis=0, keepdims=True)
    line = index_grid((8, R), 0)
    table = jnp.zeros((8, R), F32)
    rows = (slot0, slot1, prob[...] * jax.nn.sigmoid(gap), prob[...] * jax.nn.sigmoid(-gap), gid, pos)
    for at, value in enumerate(rows):
        table = jnp.where(line == at, value, table)
    info_t[...] = table.T

    def norm(b, c):
        rows = pl.ds(pl.multiple_of(b * step, step), step)
        v = tokens[rows, :].astype(F32)
        scale = lax.rsqrt(jnp.mean(v * v, axis=1, keepdims=True) + EPSILON)
        part = tokens[rows, pl.ds(pl.multiple_of(tpi * Dt, Dt), Dt)].astype(F32)
        normed[rows, :] = (part * scale).astype(BF16)
        return c

    for k, load in enumerate(loads[7:]):
        load.wait()
        if k == len(strips) - 1:
            for late in loads[:3]:
                late.start()
        lax.fori_loop(k * strip // step, (k + 1) * strip // step, norm, 0)

    def choose(q):
        pick = jnp.where((index_grid((W, R), 0) == pos) & (gid == q.astype(F32)), 1.0, 0.0)
        info_q = dot(table, pick, ((1,), (1,)), precision=lax.Precision.HIGHEST)
        return dot(pick[:Rg].astype(BF16), normed[...]).astype(BF16), info_q

    for q in others:
        s1s[q], i1s[q] = choose(q)
    pl.semaphore_wait(barrier, n - 1 + T - 1)

    def rows_to(q):
        return [
            send(a.at[q], b.at[g, side], snd.at[q], rcv.at[g, side], fs=q * EPG + half * side_for(q, g) + lane)
            for a, b, snd, rcv in ((i1s, i1r, i1_snd, i1_rcv), (s1s, s1r, s1_snd, s1_rcv))
        ]

    def rows_from(h, k):
        return [
            send(a.at[h], b.at[h, k], snd.at[h], rcv.at[h, k], fs=h * EPG)
            for a, b, snd, rcv in ((i1s, i1r, i1_snd, i1_rcv), (s1s, s1r, s1_snd, s1_rcv))
        ]

    def slots_to(h, k, origin, p):
        return send(
            s2s.at[h, k, slots(p)], x.at[tpi, h, slots(origin)], s2_snd.at[h, k], s2_rcv.at[h, origin // half],
            fs=g * EPG + p,
        )

    def dispatch(h, k, origin):
        slot_q = i1r[h, k]
        grid = index_grid((S, Rg), 0)
        spread = (grid == slot_q[0:1, :Rg]) | (grid == slot_q[1:2, :Rg])
        s2s[h, k] = dot(jnp.where(spread, 1.0, 0.0).astype(BF16), s1r[h, k]).astype(BF16)
        for j in range(1, EPG):
            slots_to(h, k, origin, partner(i, j, EPG)).start()
        x[tpi, h, slots(origin), :] = s2s[h, k, slots(i), :]

    def selection(h, k):
        cols = i1r[h, k].T[:Rg]
        grid = index_grid((Rg, S), 1)
        for c in range(TOP):
            sel[h, k, c] = jnp.where(grid == cols[:, c : c + 1], 1.0, 0.0).astype(BF16)

    for q in others:
        for copy in rows_to(q):
            copy.start()
    s1r[g, 0], i1r[g, 0] = choose(g)
    loads[6].wait()
    dispatch(g, 0, i)
    cast_weights(0, w_gate, True)
    send_weights(0, new_gate, near)
    cast_weights(1, w_up, True)
    send_weights(1, new_up, near)
    send_weights(0, new_gate, far)
    send_weights(1, new_up, far)
    cast_weights(2, w_down, False)
    for m, dst in enumerate((new_gate, new_up, new_down)):
        dst[block(me), :] = wb[m, me]

    for h in others:

        @pl.when(relays(h))
        def _():
            for k in origins(h):
                for copy in rows_from(h, k):
                    copy.wait_recv()
                dispatch(h, k, k * half + lane)

    send_weights(2, new_down, near)

    @pl.when(jnp.logical_not(outer))
    def _():
        send_weights(2, new_down, [b + j for b in range(EPG, n, EPG) for j in (*range(half, EPG), *range(half))])


    for h in others:

        @pl.when(relays(h))
        def _():
            for k in range(SIDES):
                selection(h, k)

        grid = index_grid((R, Rg), 1)
        here = (grid == info_t[:, 5:6]) & (info_t[:, 4:5] == h.astype(F32))
        place[h] = jnp.where(here, 1.0, 0.0).astype(BF16)
    selection(g, 0)
    grid = index_grid((R, Rg), 1)
    here = (grid == info_t[:, 5:6]) & (info_t[:, 4:5] == g.astype(F32))
    place[g] = jnp.where(here, 1.0, 0.0).astype(BF16)

    part = half * cap

    def portion(k):
        return pl.ds(pl.multiple_of(k * part, part), part)

    def shared(t, h, k, o):
        return send(
            x.at[t, h, portion(k)], x.at[t, h, portion(k)], tp_snd.at[h, k, o - 1], tp_rcv.at[h, k, o - 1],
            tp=(tpi + o) % T,
        )

    def take(ref, snd, rcv, full, count):
        for missing in (0, 1):

            @pl.when(full if missing == 0 else jnp.logical_not(full))
            def _():
                rows = ref.at[pl.ds(0, (count - missing) * cap)]
                send(rows, rows, snd, rcv, fs=me).wait_recv()

    def exchange(h, k, whole):
        take(x.at[tpi, h], s2_snd.at[h, k], s2_rcv.at[h, k], whole, half)
        for o in range(1, T):
            shared(tpi, h, k, o).start()

    def exchanged(h, k):
        for o in range(1, T):
            shared((tpi + T - o) % T, h, k, o).wait_recv()

    def apply_experts(h, k):
        rows = portion(k)
        gate_pre = up_pre = 0.0
        for t in range(T):
            piece = x[t, h, rows, :]
            gate_pre += dot(piece, new_gate[t * Dt : (t + 1) * Dt, :])
            up_pre += dot(piece, new_up[t * Dt : (t + 1) * Dt, :])
        hid[h, rows, :] = (gate_pre / (1.0 + jnp.exp(-gate_pre)) * up_pre).astype(BF16)

    stores = [
        pltpu.make_async_copy(src, dst, out_sem.at[k])
        for k, (src, dst) in enumerate(((new_gate, gate_out), (new_up, up_out), (new_down, down_out)))
    ]
    for k in range(SIDES):
        exchange(g, k, side != k)
    blocks(0, new_gate, me, n - 1).wait_recv()
    stores[0].start()
    for at in range(SIDES):
        for h in others:
            exchange(h, origins(h)[at], jnp.logical_not(relays(h)))
        @pl.when(outer)
        def _():
            send_weights(2, new_down, [[EPG], range(EPG + 1, n)][at])

    blocks(1, new_up, me, n - 1).wait_recv()
    stores[1].start()
    for k in range(SIDES):
        exchanged(g, k)
        apply_experts(g, k)
    for at in range(SIDES):
        for h in others:
            exchanged(h, origins(h)[at])
            apply_experts(h, origins(h)[at])

    def partial(h, c, o, t):
        return send(ps.at[o, c, h], pr.at[o, c, h], p_snd.at[0], p_rcv.at[c, h, o - 1], tp=t)

    def sum_units(t, o, c, h):
        rows = pl.ds(pl.multiple_of(t * Dt + c * Dc, Dc), Dc)
        ps[o, c, h] = dot(hid[h], new_down[rows, :], ((1,), (1,))).astype(BF16)

        @pl.when(t != tpi)
        def _():
            partial(h, c, o, t).start()

    def return_to(h, c, k, origin, p, q):
        return send(
            eo.at[c, h, slots(origin)], ret.at[c, h, k, slots(q)], r_snd.at[h], r_rcv.at[c, h, k],
            fs=g * EPG + p,
        )

    def total_units(c, h):
        total = ps[0, c, h].astype(F32)
        for o in range(1, T):
            partial(h, c, o, (tpi + o) % T).wait_recv()
            total += pr[o, c, h].astype(F32)
        eo[c, h] = total.astype(BF16)

    def hand_back_other(c, h):
        total_units(c, h)
        at = half * side_for(g, h)
        for k in range(SIDES):

            @pl.when(relays(h))
            def _():
                ret[c, h, k, slots(i), :] = eo[c, h, slots(k * half + lane), :]

            @pl.when(jnp.logical_not(relays(h)))
            def _():
                return_to(h, c, k, k * half + lane, at + lane, i).start()

            for j in range(1, half):
                l = partner(lane, j, half)
                return_to(h, c, k, k * half + l, at + l, i).start()

    def hand_back_own(c):
        total_units(c, g)
        for j in range(1, EPG):
            p = partner(i, j, EPG)
            return_to(g, c, 0, p, p, i).start()
        ret[c, g, 0, slots(i), :] = eo[c, g, slots(i), :]

    def result_to(h, c, k, q):
        return send(
            ms.at[c, h, k], fin.at[c, q], f_snd.at[h, k], f_rcv.at[c, q], fs=h * EPG + k * half + lane
        )

    def mix(c, h, k):
        rows = ret.at[c, h, k, pl.ds(0, (EPG - 1) * cap)]
        send(rows, rows, r_snd.at[h], r_rcv.at[c, h, k], fs=me).wait_recv()
        cols = i1r[h, k].T[:Rg]
        outs = ret[c, h, k]
        return (cols[:, 2:3] * dot(sel[h, k, 0], outs) + cols[:, 3:4] * dot(sel[h, k, 1], outs)).astype(BF16)

    def mix_other(c, h):
        @pl.when(relays(h))
        def _():
            for k in range(SIDES):
                ms[c, h, k] = mix(c, h, k)
                result_to(h, c, k, g).start()

    first = me // per_part
    for k in range(T):
        t = (first + k) % T
        if k == 0:
            blocks(2, new_down, me, per_part - 1).wait_recv()
        else:
            blocks(2, new_down, t * per_part, per_part).wait_recv()
        if k == T - 1:
            stores[2].start()
        for h in others:
            for c in range(C):
                sum_units(t, (t - tpi + T) % T, c, h)

        @pl.when(t == tpi)
        def _():
            for h in others:
                for c in range(C):
                    hand_back_other(c, h)

        for c in range(C):
            sum_units(t, (t - tpi + T) % T, c, g)

        @pl.when(t == tpi)
        def _():
            for c in range(C):
                hand_back_own(c)


    for h in others:
        for c in range(C):
            mix_other(c, h)

    for c in range(C):
        fin[c, g] = mix(c, g, 0)
        total = dot(place[g], fin[c, g])
        for q in others:
            result_to(q, c, 0, q).wait_recv()
            total += dot(place[q], fin[c, q])
        mixed[:, c * Dc : (c + 1) * Dc] = total.astype(BF16)
        stores.append(
            pltpu.make_async_copy(
                mixed.at[:, c * Dc : (c + 1) * Dc], mixed_out.at[:, c * Dc : (c + 1) * Dc], out_sem.at[3 + c]
            )
        )
        stores[-1].start()
    for store in stores:
        store.wait()

    def drain(ref, sem):
        send(ref, ref, sem, sem, fs=me).wait_send()

    for m in range(3):
        drain(wb.at[m, pl.ds(0, n - 1)], w_snd.at[m])
    sent = pl.ds(0, (EPG - 1) * cap)
    drain(s2s.at[g, 0, sent], s2_snd.at[g, 0])
    drain(eo.at[pl.ds(0, C), g, sent], r_snd.at[g])
    if T > 1:
        drain(ps.at[pl.ds(1, T - 1)], p_snd.at[0])
    for h in (*others, g):
        for k in range(SIDES):
            for o in range(1, T):
                shared(tpi, h, k, o).wait_send()
    for h in others:
        for copy in rows_to(h):
            copy.wait_send()

        @pl.when(relays(h))
        def _():
            drain(eo.at[pl.ds(0, C), h, pl.ds(0, (EPG - SIDES) * cap)], r_snd.at[h])
            for k in range(SIDES):
                drain(s2s.at[h, k, sent], s2_snd.at[h, k])
                drain(ms.at[pl.ds(0, C), h, k], f_snd.at[h, k])

        @pl.when(jnp.logical_not(relays(h)))
        def _():
            drain(eo.at[pl.ds(0, C), h], r_snd.at[h])


def hand_over(count, *refs):
    sources, results, rooms = refs[:4], refs[4:8], refs[8:12]
    arrived, left = refs[12:]
    into, out = [], []
    for a, (source, room, result) in enumerate(zip(sources, rooms, results)):
        height = source.shape[0] // count
        for b in range(count):
            rows = pl.ds(b * height, height)
            into.append(pltpu.make_async_copy(source.at[rows], room.at[rows], arrived.at[a, b]))
            out.append(pltpu.make_async_copy(room.at[rows], result.at[rows], left.at[a, b]))
    for copy in into:
        copy.start()
    for first, second in zip(into, out):
        first.wait()
        second.start()
    for copy in out:
        copy.wait()


def local(tokens, norm_gain, w_gate, w_up, w_down, route_expert, group_prob, pair_logit):
    n, T = lax.axis_size("fs"), lax.axis_size("tp")
    R, D = tokens.shape
    F = w_gate.shape[2]
    G = n // EPG
    Rg, cap, Dt = R // G, TOP * R // n, D // T
    S, W = EPG * cap, max(Rg, 128)
    Dc = min(Dt, max(Dt // CHUNKS, 128))
    C = Dt // Dc
    hbm = pl.BlockSpec(memory_space=pl.ANY)
    sem = pltpu.SemaphoreType.DMA
    weights = jax.ShapeDtypeStruct((D, F), BF16)
    shapes = [weights, weights, weights, jax.ShapeDtypeStruct((R, Dt), BF16)]
    results = pl.pallas_call(
        functools.partial(kernel, n, T),
        out_shape=shapes,
        in_specs=[hbm] * 8,
        out_specs=[hbm] * 4,
        scratch_shapes=[
            pltpu.VMEM((TOP, R), jnp.int32),
            pltpu.VMEM((1, D // n), F32),
            pltpu.VMEM((1, R), F32),
            pltpu.VMEM((TOP, R), F32),
            pltpu.VMEM((R, D), BF16),
            pltpu.VMEM(w_gate.shape, F32),
            pltpu.VMEM(w_up.shape, F32),
            pltpu.VMEM(w_down.shape, F32),
            pltpu.VMEM((D, F), BF16),
            pltpu.VMEM((D, F), BF16),
            pltpu.VMEM((D, F), BF16),
            pltpu.VMEM((R, Dt), BF16),
            pltpu.VMEM((3, n, D // n, F), BF16),
            pltpu.VMEM((R, Dt), BF16),
            pltpu.VMEM((R, 8), F32),
            pltpu.VMEM((G, Rg, Dt), BF16),
            pltpu.VMEM((G, 8, W), F32),
            pltpu.VMEM((G, SIDES, Rg, Dt), BF16),
            pltpu.VMEM((G, SIDES, 8, W), F32),
            pltpu.VMEM((G, SIDES, S, Dt), BF16),
            pltpu.VMEM((T, G, S, Dt), BF16),
            pltpu.VMEM((G, SIDES, TOP, Rg, S), BF16),
            pltpu.VMEM((G, R, Rg), BF16),
            pltpu.VMEM((G, S, F), BF16),
            pltpu.VMEM((T, C, G, S, Dc), BF16),
            pltpu.VMEM((T, C, G, S, Dc), BF16),
            pltpu.VMEM((C, G, S, Dc), BF16),
            pltpu.VMEM((C, G, SIDES, S, Dc), BF16),
            pltpu.VMEM((C, G, SIDES, Rg, Dc), BF16),
            pltpu.VMEM((C, G, Rg, Dc), BF16),
            sem((7 + STRIPS,)), sem((3 + C,)),
            sem((3,)), sem((2 + T,)),
            sem((G,)), sem((G, SIDES)), sem((G,)), sem((G, SIDES)),
            sem((G, SIDES)), sem((G, SIDES)),
            sem((G, SIDES, max(T - 1, 1))), sem((G, SIDES, max(T - 1, 1))), sem((1,)), sem((C, G, max(T - 1, 1))),
            sem((G,)), sem((C, G, SIDES)),
            sem((G, SIDES)), sem((C, G)),
        ],
        compiler_params=pltpu.CompilerParams(
            collective_id=0, has_side_effects=True, vmem_limit_bytes=VMEM_LIMIT
        ),
    )(
        route_expert.T, norm_gain[None, :], group_prob[None, :], pair_logit.T,
        tokens, w_gate, w_up, w_down,
    )
    parts = 2
    gate, up, down, mixed = pl.pallas_call(
        functools.partial(hand_over, parts),
        out_shape=shapes,
        in_specs=[hbm] * 4,
        out_specs=[hbm] * 4,
        scratch_shapes=[pltpu.VMEM(s.shape, s.dtype) for s in shapes] + [sem((4, parts)), sem((4, parts))],
    )(*results)
    return gate[None], up[None], down[None], mixed


def solution(mesh):
    placed = (
        P("fs", None),
        P("fs"),
        P(None, "fs", "tp"),
        P(None, "fs", "tp"),
        P(None, "fs", "tp"),
        P("fs", None),
        P("fs"),
        P("fs", None),
    )
    return jax.shard_map(
        local,
        mesh=mesh,
        in_specs=placed,
        out_specs=(P("fs", None, "tp"), P("fs", None, "tp"), P("fs", None, "tp"), P("fs", "tp")),
        check_vma=False,
    )
```

```python
import functools

import jax
import jax.numpy as jnp
from jax import lax
from jax.experimental import pallas as pl
from jax.experimental.pallas import tpu as pltpu
from jax.sharding import PartitionSpec as P

EPG = 8
SIDES = 2
TOP = 2
EPSILON = 1e-06
MESH = pl.DeviceIdType.MESH
F32, BF16 = jnp.float32, jnp.bfloat16
CHUNKS = 4
STRIPS = 4
VMEM_LIMIT = 62 * 1024 * 1024


def index_grid(shape, dim):
    return lax.broadcasted_iota(jnp.int32, shape, dim).astype(F32)


def dot(a, b, contract=((1,), (0,)), **kw):
    return lax.dot_general(a, b, (contract, ((), ())), preferred_element_type=F32, **kw)


def send(src, dst, send_sem, recv_sem, **where):
    return pltpu.make_async_remote_copy(
        src_ref=src, dst_ref=dst, send_sem=send_sem, recv_sem=recv_sem, device_id=where, device_id_type=MESH
    )


def partner(me, j, n):
    if n & (n - 1):
        return (me + j) % n
    p, bit = 0, 1
    while bit < n:
        here = (me // bit) % 2
        p = p + bit * (1 - here if j & bit else here)
        bit *= 2
    return p


def kernel(
    n, T, ids_in, gain_in, prob_in, logit_in, tokens_in, gate_in, up_in, down_in, gate_out, up_out, down_out, mixed_out,
    ids, gain, prob, logit, tokens, w_gate, w_up, w_down, new_gate, new_up, new_down, mixed,
    wb, normed, info_t, s1s, i1s, s1r, i1r, s2s, x, sel, place, hid, ps, pr, eo, ret, ms, fin,
    in_sem, out_sem, w_snd, w_rcv, s1_snd, s1_rcv, i1_snd, i1_rcv, s2_snd, s2_rcv, tp_snd, tp_rcv,
    p_snd, p_rcv, r_snd, r_rcv, f_snd, f_rcv,
):
    me, tpi = lax.axis_index("fs"), lax.axis_index("tp")
    R, D = tokens.shape
    G = n // EPG
    g, i = me // EPG, me % EPG
    Rg, cap, Dt, K = R // G, TOP * R // n, D // T, D // n
    S = EPG * cap
    W = i1s.shape[2]
    C, Dc = ps.shape[1], ps.shape[4]
    half = EPG // SIDES
    lane, side = i % half, i // half
    others = [(g + 1 + k) % G for k in range(G - 1)]

    def side_for(q, h):
        return (h - q + G) // G

    def relays(h):
        return side == side_for(g, h)

    def outside(h):
        return (SIDES * h) // G

    def origins(h):
        return [(outside(h) + k) % SIDES for k in range(SIDES)]

    outer = side == outside(g)

    barrier = pltpu.get_barrier_semaphore()

    step = min(R, 64)
    strip = max(R // STRIPS, step)
    strips = [pl.ds(k * strip, strip) for k in range(R // strip)]
    loads = [
        pltpu.make_async_copy(src, dst, in_sem.at[k])
        for k, (src, dst) in enumerate(
            (
                (gate_in, w_gate), (up_in, w_up), (down_in, w_down),
                (ids_in, ids), (logit_in, logit), (prob_in, prob), (gain_in, gain),
                *((tokens_in.at[rows], tokens.at[rows]) for rows in strips),
            )
        )
    ]
    for load in loads[3:]:
        load.start()

    def greet(k, c):
        pl.semaphore_signal(barrier, inc=1, device_id={"fs": (me + k) % n}, device_id_type=MESH)
        return c

    lax.fori_loop(1, n, greet, 0)
    for o in range(1, T):
        pl.semaphore_signal(barrier, inc=1, device_id={"tp": (tpi + o) % T}, device_id_type=MESH)

    def block(p):
        return pl.ds(pl.multiple_of(p * K, K), K)

    def slots(p):
        return pl.ds(pl.multiple_of(p * cap, cap), cap)

    def spread_gain():
        diagonal = index_grid((K, K), 0) == index_grid((K, K), 1)
        return jnp.sum(jnp.where(diagonal, gain[...], 0.0), axis=1, keepdims=True)

    def cast_weights(m, src, scaled):
        gains = spread_gain() if scaled else None

        def cast(p, c):
            v = src[p]
            wb[m, p] = (v * gains if scaled else v).astype(BF16)
            return c

        loads[m].wait()
        lax.fori_loop(0, n, cast, 0)

    per_part = n // T

    def arrival(m, p):
        return w_rcv.at[m + p // per_part if m == 2 else m]

    def send_weights(m, dst, order):
        for j in order:
            p = partner(me, j, n)
            send(wb.at[m, p], dst.at[block(me)], w_snd.at[m], arrival(m, me), fs=p).start()

    near, far = range(1, EPG), range(EPG, n)

    def blocks(m, dst, p, count):
        rows = dst.at[pl.ds(0, count * K)]
        return send(rows, rows, w_snd.at[m], arrival(m, p), fs=p)

    for load in loads[3:6]:
        load.wait()
    id0, id1 = ids[0:1, :].astype(F32), ids[1:2, :].astype(F32)
    gap = logit[0:1, :] - logit[1:2, :]
    gid = jnp.floor(id0 * (1.0 / EPG))
    experts = index_grid((n, R), 0)
    m0, m1 = experts == id0, experts == id1
    before = jnp.where(index_grid((R, R), 0) < index_grid((R, R), 1), 1.0, 0.0).astype(BF16)
    rank = dot(jnp.where(m0 | m1, 1.0, 0.0).astype(BF16), before)
    in_group = index_grid((max(G, 16), R), 0) == gid
    group_rank = dot(jnp.where(in_group, 1.0, 0.0).astype(BF16), before)
    slot0 = jnp.sum(jnp.where(m0, rank, 0.0), axis=0, keepdims=True) + (id0 - EPG * gid) * cap
    slot1 = jnp.sum(jnp.where(m1, rank, 0.0), axis=0, keepdims=True) + (id1 - EPG * gid) * cap
    pos = jnp.sum(jnp.where(in_group, group_rank, 0.0), axis=0, keepdims=True)
    line = index_grid((8, R), 0)
    table = jnp.zeros((8, R), F32)
    rows = (slot0, slot1, prob[...] * jax.nn.sigmoid(gap), prob[...] * jax.nn.sigmoid(-gap), gid, pos)
    for at, value in enumerate(rows):
        table = jnp.where(line == at, value, table)
    info_t[...] = table.T

    def norm(b, c):
        rows = pl.ds(pl.multiple_of(b * step, step), step)
        v = tokens[rows, :].astype(F32)
        scale = lax.rsqrt(jnp.mean(v * v, axis=1, keepdims=True) + EPSILON)
        part = tokens[rows, pl.ds(pl.multiple_of(tpi * Dt, Dt), Dt)].astype(F32)
        normed[rows, :] = (part * scale).astype(BF16)
        return c

    for k, load in enumerate(loads[7:]):
        load.wait()
        if k == len(strips) - 1:
            for late in loads[:3]:
                late.start()
        lax.fori_loop(k * strip // step, (k + 1) * strip // step, norm, 0)

    def choose(q):
        pick = jnp.where((index_grid((W, R), 0) == pos) & (gid == q.astype(F32)), 1.0, 0.0)
        info_q = dot(table, pick, ((1,), (1,)), precision=lax.Precision.HIGHEST)
        return dot(pick[:Rg].astype(BF16), normed[...]).astype(BF16), info_q

    for q in others:
        s1s[q], i1s[q] = choose(q)
    pl.semaphore_wait(barrier, n - 1 + T - 1)

    def rows_to(q):
        return [
            send(a.at[q], b.at[g, side], snd.at[q], rcv.at[g, side], fs=q * EPG + half * side_for(q, g) + lane)
            for a, b, snd, rcv in ((i1s, i1r, i1_snd, i1_rcv), (s1s, s1r, s1_snd, s1_rcv))
        ]

    def rows_from(h, k):
        return [
            send(a.at[h], b.at[h, k], snd.at[h], rcv.at[h, k], fs=h * EPG)
            for a, b, snd, rcv in ((i1s, i1r, i1_snd, i1_rcv), (s1s, s1r, s1_snd, s1_rcv))
        ]

    def slots_to(h, k, origin, p):
        return send(
            s2s.at[h, k, slots(p)], x.at[tpi, h, slots(origin)], s2_snd.at[h, k], s2_rcv.at[h, origin // half],
            fs=g * EPG + p,
        )

    def dispatch(h, k, origin):
        slot_q = i1r[h, k]
        grid = index_grid((S, Rg), 0)
        spread = (grid == slot_q[0:1, :Rg]) | (grid == slot_q[1:2, :Rg])
        s2s[h, k] = dot(jnp.where(spread, 1.0, 0.0).astype(BF16), s1r[h, k]).astype(BF16)
        for j in range(1, EPG):
            slots_to(h, k, origin, partner(i, j, EPG)).start()
        x[tpi, h, slots(origin), :] = s2s[h, k, slots(i), :]

    def selection(h, k):
        cols = i1r[h, k].T[:Rg]
        grid = index_grid((Rg, S), 1)
        for c in range(TOP):
            sel[h, k, c] = jnp.where(grid == cols[:, c : c + 1], 1.0, 0.0).astype(BF16)

    for q in others:
        for copy in rows_to(q):
            copy.start()
    s1r[g, 0], i1r[g, 0] = choose(g)
    loads[6].wait()
    dispatch(g, 0, i)
    cast_weights(0, w_gate, True)
    send_weights(0, new_gate, near)
    cast_weights(1, w_up, True)
    send_weights(1, new_up, near)
    send_weights(0, new_gate, far)
    send_weights(1, new_up, far)
    cast_weights(2, w_down, False)
    for m, dst in enumerate((new_gate, new_up, new_down)):
        dst[block(me), :] = wb[m, me]

    for h in others:

        @pl.when(relays(h))
        def _():
            for k in origins(h):
                for copy in rows_from(h, k):
                    copy.wait_recv()
                dispatch(h, k, k * half + lane)

    send_weights(2, new_down, near)

    @pl.when(jnp.logical_not(outer))
    def _():
        send_weights(2, new_down, [b + j for b in range(EPG, n, EPG) for j in (*range(half, EPG), *range(half))])


    for h in others:

        @pl.when(relays(h))
        def _():
            for k in range(SIDES):
                selection(h, k)

        grid = index_grid((R, Rg), 1)
        here = (grid == info_t[:, 5:6]) & (info_t[:, 4:5] == h.astype(F32))
        place[h] = jnp.where(here, 1.0, 0.0).astype(BF16)
    selection(g, 0)
    grid = index_grid((R, Rg), 1)
    here = (grid == info_t[:, 5:6]) & (info_t[:, 4:5] == g.astype(F32))
    place[g] = jnp.where(here, 1.0, 0.0).astype(BF16)

    part = half * cap

    def portion(k):
        return pl.ds(pl.multiple_of(k * part, part), part)

    def shared(t, h, k, o):
        return send(
            x.at[t, h, portion(k)], x.at[t, h, portion(k)], tp_snd.at[h, k, o - 1], tp_rcv.at[h, k, o - 1],
            tp=(tpi + o) % T,
        )

    def take(ref, snd, rcv, full, count):
        for missing in (0, 1):

            @pl.when(full if missing == 0 else jnp.logical_not(full))
            def _():
                rows = ref.at[pl.ds(0, (count - missing) * cap)]
                send(rows, rows, snd, rcv, fs=me).wait_recv()

    def exchange(h, k, whole):
        take(x.at[tpi, h], s2_snd.at[h, k], s2_rcv.at[h, k], whole, half)
        for o in range(1, T):
            shared(tpi, h, k, o).start()

    def exchanged(h, k):
        for o in range(1, T):
            shared((tpi + T - o) % T, h, k, o).wait_recv()

    def apply_experts(h, k):
        rows = portion(k)
        gate_pre = up_pre = 0.0
        for t in range(T):
            piece = x[t, h, rows, :]
            gate_pre += dot(piece, new_gate[t * Dt : (t + 1) * Dt, :])
            up_pre += dot(piece, new_up[t * Dt : (t + 1) * Dt, :])
        hid[h, rows, :] = (gate_pre / (1.0 + jnp.exp(-gate_pre)) * up_pre).astype(BF16)

    stores = [
        pltpu.make_async_copy(src, dst, out_sem.at[k])
        for k, (src, dst) in enumerate(((new_gate, gate_out), (new_up, up_out), (new_down, down_out)))
    ]
    for k in range(SIDES):
        exchange(g, k, side != k)
    blocks(0, new_gate, me, n - 1).wait_recv()
    stores[0].start()
    for at in range(SIDES):
        for h in others:
            exchange(h, origins(h)[at], jnp.logical_not(relays(h)))
        @pl.when(outer)
        def _():
            send_weights(2, new_down, [range(EPG, EPG + 2), range(EPG + 2, n)][at])

    blocks(1, new_up, me, n - 1).wait_recv()
    stores[1].start()
    for k in range(SIDES):
        exchanged(g, k)
        apply_experts(g, k)
    for at in range(SIDES):
        for h in others:
            exchanged(h, origins(h)[at])
            apply_experts(h, origins(h)[at])

    def partial(h, c, o, t):
        return send(ps.at[o, c, h], pr.at[o, c, h], p_snd.at[0], p_rcv.at[c, h, o - 1], tp=t)

    def sum_units(t, o, c, h):
        rows = pl.ds(pl.multiple_of(t * Dt + c * Dc, Dc), Dc)
        ps[o, c, h] = dot(hid[h], new_down[rows, :], ((1,), (1,))).astype(BF16)

        @pl.when(t != tpi)
        def _():
            partial(h, c, o, t).start()

    def return_to(h, c, k, origin, p, q):
        return send(
            eo.at[c, h, slots(origin)], ret.at[c, h, k, slots(q)], r_snd.at[h], r_rcv.at[c, h, k],
            fs=g * EPG + p,
        )

    def total_units(c, h):
        total = ps[0, c, h].astype(F32)
        for o in range(1, T):
            partial(h, c, o, (tpi + o) % T).wait_recv()
            total += pr[o, c, h].astype(F32)
        eo[c, h] = total.astype(BF16)

    def hand_back_other(c, h):
        total_units(c, h)
        at = half * side_for(g, h)
        for k in range(SIDES):

            @pl.when(relays(h))
            def _():
                ret[c, h, k, slots(i), :] = eo[c, h, slots(k * half + lane), :]

            @pl.when(jnp.logical_not(relays(h)))
            def _():
                return_to(h, c, k, k * half + lane, at + lane, i).start()

            for j in range(1, half):
                l = partner(lane, j, half)
                return_to(h, c, k, k * half + l, at + l, i).start()

    def hand_back_own(c):
        total_units(c, g)
        for j in range(1, EPG):
            p = partner(i, j, EPG)
            return_to(g, c, 0, p, p, i).start()
        ret[c, g, 0, slots(i), :] = eo[c, g, slots(i), :]

    def result_to(h, c, k, q):
        return send(
            ms.at[c, h, k], fin.at[c, q], f_snd.at[h, k], f_rcv.at[c, q], fs=h * EPG + k * half + lane
        )

    def mix(c, h, k):
        rows = ret.at[c, h, k, pl.ds(0, (EPG - 1) * cap)]
        send(rows, rows, r_snd.at[h], r_rcv.at[c, h, k], fs=me).wait_recv()
        cols = i1r[h, k].T[:Rg]
        outs = ret[c, h, k]
        return (cols[:, 2:3] * dot(sel[h, k, 0], outs) + cols[:, 3:4] * dot(sel[h, k, 1], outs)).astype(BF16)

    def mix_other(c, h):
        @pl.when(relays(h))
        def _():
            for k in range(SIDES):
                ms[c, h, k] = mix(c, h, k)
                result_to(h, c, k, g).start()

    first = me // per_part
    for k in range(T):
        t = (first + k) % T
        if k == 0:
            blocks(2, new_down, me, per_part - 1).wait_recv()
        else:
            blocks(2, new_down, t * per_part, per_part).wait_recv()
        if k == T - 1:
            stores[2].start()
        for h in others:
            for c in range(C):
                sum_units(t, (t - tpi + T) % T, c, h)

        @pl.when(t == tpi)
        def _():
            for h in others:
                for c in range(C):
                    hand_back_other(c, h)

        for c in range(C):
            sum_units(t, (t - tpi + T) % T, c, g)

        @pl.when(t == tpi)
        def _():
            for c in range(C):
                hand_back_own(c)


    for h in others:
        for c in range(C):
            mix_other(c, h)

    for c in range(C):
        fin[c, g] = mix(c, g, 0)
        total = dot(place[g], fin[c, g])
        for q in others:
            result_to(q, c, 0, q).wait_recv()
            total += dot(place[q], fin[c, q])
        mixed[:, c * Dc : (c + 1) * Dc] = total.astype(BF16)
        stores.append(
            pltpu.make_async_copy(
                mixed.at[:, c * Dc : (c + 1) * Dc], mixed_out.at[:, c * Dc : (c + 1) * Dc], out_sem.at[3 + c]
            )
        )
        stores[-1].start()
    for store in stores:
        store.wait()

    def drain(ref, sem):
        send(ref, ref, sem, sem, fs=me).wait_send()

    for m in range(3):
        drain(wb.at[m, pl.ds(0, n - 1)], w_snd.at[m])
    sent = pl.ds(0, (EPG - 1) * cap)
    drain(s2s.at[g, 0, sent], s2_snd.at[g, 0])
    drain(eo.at[pl.ds(0, C), g, sent], r_snd.at[g])
    if T > 1:
        drain(ps.at[pl.ds(1, T - 1)], p_snd.at[0])
    for h in (*others, g):
        for k in range(SIDES):
            for o in range(1, T):
                shared(tpi, h, k, o).wait_send()
    for h in others:
        for copy in rows_to(h):
            copy.wait_send()

        @pl.when(relays(h))
        def _():
            drain(eo.at[pl.ds(0, C), h, pl.ds(0, (EPG - SIDES) * cap)], r_snd.at[h])
            for k in range(SIDES):
                drain(s2s.at[h, k, sent], s2_snd.at[h, k])
                drain(ms.at[pl.ds(0, C), h, k], f_snd.at[h, k])

        @pl.when(jnp.logical_not(relays(h)))
        def _():
            drain(eo.at[pl.ds(0, C), h], r_snd.at[h])


def hand_over(count, *refs):
    sources, results, rooms = refs[:4], refs[4:8], refs[8:12]
    arrived, left = refs[12:]
    into, out = [], []
    for a, (source, room, result) in enumerate(zip(sources, rooms, results)):
        height = source.shape[0] // count
        for b in range(count):
            rows = pl.ds(b * height, height)
            into.append(pltpu.make_async_copy(source.at[rows], room.at[rows], arrived.at[a, b]))
            out.append(pltpu.make_async_copy(room.at[rows], result.at[rows], left.at[a, b]))
    for copy in into:
        copy.start()
    for first, second in zip(into, out):
        first.wait()
        second.start()
    for copy in out:
        copy.wait()


def local(tokens, norm_gain, w_gate, w_up, w_down, route_expert, group_prob, pair_logit):
    n, T = lax.axis_size("fs"), lax.axis_size("tp")
    R, D = tokens.shape
    F = w_gate.shape[2]
    G = n // EPG
    Rg, cap, Dt = R // G, TOP * R // n, D // T
    S, W = EPG * cap, max(Rg, 128)
    Dc = min(Dt, max(Dt // CHUNKS, 128))
    C = Dt // Dc
    hbm = pl.BlockSpec(memory_space=pl.ANY)
    sem = pltpu.SemaphoreType.DMA
    weights = jax.ShapeDtypeStruct((D, F), BF16)
    shapes = [weights, weights, weights, jax.ShapeDtypeStruct((R, Dt), BF16)]
    results = pl.pallas_call(
        functools.partial(kernel, n, T),
        out_shape=shapes,
        in_specs=[hbm] * 8,
        out_specs=[hbm] * 4,
        scratch_shapes=[
            pltpu.VMEM((TOP, R), jnp.int32),
            pltpu.VMEM((1, D // n), F32),
            pltpu.VMEM((1, R), F32),
            pltpu.VMEM((TOP, R), F32),
            pltpu.VMEM((R, D), BF16),
            pltpu.VMEM(w_gate.shape, F32),
            pltpu.VMEM(w_up.shape, F32),
            pltpu.VMEM(w_down.shape, F32),
            pltpu.VMEM((D, F), BF16),
            pltpu.VMEM((D, F), BF16),
            pltpu.VMEM((D, F), BF16),
            pltpu.VMEM((R, Dt), BF16),
            pltpu.VMEM((3, n, D // n, F), BF16),
            pltpu.VMEM((R, Dt), BF16),
            pltpu.VMEM((R, 8), F32),
            pltpu.VMEM((G, Rg, Dt), BF16),
            pltpu.VMEM((G, 8, W), F32),
            pltpu.VMEM((G, SIDES, Rg, Dt), BF16),
            pltpu.VMEM((G, SIDES, 8, W), F32),
            pltpu.VMEM((G, SIDES, S, Dt), BF16),
            pltpu.VMEM((T, G, S, Dt), BF16),
            pltpu.VMEM((G, SIDES, TOP, Rg, S), BF16),
            pltpu.VMEM((G, R, Rg), BF16),
            pltpu.VMEM((G, S, F), BF16),
            pltpu.VMEM((T, C, G, S, Dc), BF16),
            pltpu.VMEM((T, C, G, S, Dc), BF16),
            pltpu.VMEM((C, G, S, Dc), BF16),
            pltpu.VMEM((C, G, SIDES, S, Dc), BF16),
            pltpu.VMEM((C, G, SIDES, Rg, Dc), BF16),
            pltpu.VMEM((C, G, Rg, Dc), BF16),
            sem((7 + STRIPS,)), sem((3 + C,)),
            sem((3,)), sem((2 + T,)),
            sem((G,)), sem((G, SIDES)), sem((G,)), sem((G, SIDES)),
            sem((G, SIDES)), sem((G, SIDES)),
            sem((G, SIDES, max(T - 1, 1))), sem((G, SIDES, max(T - 1, 1))), sem((1,)), sem((C, G, max(T - 1, 1))),
            sem((G,)), sem((C, G, SIDES)),
            sem((G, SIDES)), sem((C, G)),
        ],
        compiler_params=pltpu.CompilerParams(
            collective_id=0, has_side_effects=True, vmem_limit_bytes=VMEM_LIMIT
        ),
    )(
        route_expert.T, norm_gain[None, :], group_prob[None, :], pair_logit.T,
        tokens, w_gate, w_up, w_down,
    )
    parts = 2
    gate, up, down, mixed = pl.pallas_call(
        functools.partial(hand_over, parts),
        out_shape=shapes,
        in_specs=[hbm] * 4,
        out_specs=[hbm] * 4,
        scratch_shapes=[pltpu.VMEM(s.shape, s.dtype) for s in shapes] + [sem((4, parts)), sem((4, parts))],
    )(*results)
    return gate[None], up[None], down[None], mixed


def solution(mesh):
    placed = (
        P("fs", None),
        P("fs"),
        P(None, "fs", "tp"),
        P(None, "fs", "tp"),
        P(None, "fs", "tp"),
        P("fs", None),
        P("fs"),
        P("fs", None),
    )
    return jax.shard_map(
        local,
        mesh=mesh,
        in_specs=placed,
        out_specs=(P("fs", None, "tp"), P("fs", None, "tp"), P("fs", None, "tp"), P("fs", "tp")),
        check_vma=False,
    )
```
